32 devices in a mesh: grp: 2 (over y), sp: 4 (over z), tp: 4 (over x, core).
Axes of the slice: x: 2, y: 2, z: 4, core: 2. Of those that a mesh axis runs over, the one named last changes fastest.
Arguments:
- starting_stream: bfloat16 [3072, 2048], P(('grp', 'sp'), 'tp'), parts along dimension 0, may hold values from -45 to 45
- multiplier_matrix: bfloat16 [2, 2048, 2048], P(None, 'sp', 'tp'), may hold values from -0.125 to 0.125
- memory_path_matrix: bfloat16 [2, 2048, 2048], P(None, 'sp', 'tp'), may hold values from -0.125 to 0.125
- filter_coefficients: bfloat16 [2, 4, 2048], P(None, None, 'tp'), may hold values from -3 to 3
- memory_valve_matrix: bfloat16 [2, 8, 256, 256], P(None, 'tp'), may hold values from -0.375 to 0.375
- entry_valve_matrix: bfloat16 [2, 8, 256, 256], P(None, 'tp'), may hold values from -0.375 to 0.375
- forgetting_parameters: float32 [2, 2048], P(None, 'tp'), may hold values from 3 to 15
- timestep_forgetting_multiplier: float32 [3072], P(('grp', 'sp')), parts along dimension 0, may hold values from 0.5 to 2
- spike_extra: float32 [3072, 2048], P(('grp', 'sp'), 'tp'), parts along dimension 0, may hold values from -0.7 to 0
- exit_projector_matrix: bfloat16 [2, 2048, 2048], P(None, 'tp', 'sp'), may hold values from -0.125 to 0.125
- prelude_rms_gains: float32 [2, 2048], replicated, may hold values from 0.1 to 1.9
- finishing_rms_gains: float32 [2048], P('tp'), may hold values from 0.1 to 1.9
Outputs:
- result: bfloat16 [3072, 2048], P(('grp', 'sp'), 'tp'), parts along dimension 0
The draws below stay inside these ranges and needn't reach their ends.
There are 2 independent parts, one for each index of `grp`. The reference program is written for one: setup_inputs(seed, part) draws one part's arguments, and reference() takes and returns one part's arrays. A program takes and returns all parts, laid end to end along the dimension named above; an argument that names none is the same for every part. Nothing has to cross between parts.
All inputs are finite; a program needn't handle non-finite values.
Results may differ from the reference program's by a relative error of at most 0.015.
Values may be sent and summed in bfloat16 or wider, within the bound.
A program may use at most 64 MiB of HBM per device.

```python
import math
import jax
import jax.numpy as jnp
from jax import lax

D = 2048
W = 2048
BLOCK_W = 256
BLOCKS = 8
CONV = 4
LAYERS = 2
TOK_DEV = 384
TOKENS = 1536
N_TP = 4


def draw_starting_stream(key, part):
    keys = jax.random.split(key, 3)
    columns = jnp.arange(D, dtype=jnp.float32)
    col_scale = jnp.exp(math.log(4.0) * columns / D) * jax.random.uniform(keys[1], (D,), jnp.float32, 0.7, 1.4)
    row_scale = jnp.exp(jax.random.uniform(keys[2], (TOKENS, 1), jnp.float32, math.log(0.5), math.log(2.0)))
    base = jnp.clip(jax.random.normal(keys[0], (TOKENS, D), jnp.float32), -4.0, 4.0)
    return (base * col_scale[None, :] * row_scale).astype(jnp.bfloat16)


def draw_forgetting_parameters(key, part):
    keys = jax.random.split(key, 3)
    share_fast = 0.5
    fast = jax.random.bernoulli(keys[0], share_fast, (LAYERS, W))
    fast_rate = jnp.exp(jax.random.uniform(keys[1], (LAYERS, W), jnp.float32, math.log(0.01), math.log(0.03)))
    slow_rate = jnp.exp(jax.random.uniform(keys[2], (LAYERS, W), jnp.float32, math.log(0.1), math.log(0.5))) / (4.0 * TOKENS)
    rate = jnp.where(fast, fast_rate, slow_rate)
    return -jnp.log(jnp.expm1(rate))


def draw_timestep_forgetting_multiplier(key, part):
    counted = TOKENS // TOK_DEV
    values = jnp.exp(jax.random.uniform(key, (counted,), jnp.float32, math.log(0.5), math.log(2.0)))
    return jnp.repeat(values, TOK_DEV, total_repeat_length=TOKENS)


def draw_spike_extra(key, part):
    keys = jax.random.split(key, 2)
    spots = jax.random.randint(keys[0], (4,), 0, TOKENS)
    places = jnp.arange(TOKENS, dtype=jnp.int32)
    struck = jnp.any(places[:, None] == spots[None, :], axis=1)
    depth = jnp.log(jax.random.uniform(keys[1], (TOKENS, W), jnp.float32, 0.5, 0.8))
    return jnp.where(struck[:, None], depth, 0.0)


def levels(own_key, dims, shards, least, high):
    factor_of, own = 1.0, jax.random.fold_in(own_key, 6)
    for axis_at, shards_of in shards:
        draws = jnp.exp(jax.random.uniform(jax.random.fold_in(own, axis_at), (shards_of,), jnp.float32, least / len(shards), high / len(shards)))
        factor_of = factor_of * jnp.repeat(draws, dims[axis_at] // shards_of).reshape([-1 if axis == axis_at else 1 for axis in range(len(dims))])
    return factor_of


def gaussian(stream_key, shape, scale, reach, shards=(), held_as=jnp.bfloat16):
    level = levels(stream_key, shape, shards, -0.22, 0.18) if shards else 1.0
    array = jax.random.normal(stream_key, shape, jnp.float32) * scale * level
    return jnp.minimum(jnp.maximum(array, -reach), reach).astype(held_as)


def setup_inputs(seed: int = 0, part: int = 0) -> dict:
    seeds = jax.random.split(jax.random.key(seed), 13)
    part_keys = jax.random.split(jax.random.fold_in(seeds[12], part), 13)
    return {
        "starting_stream": draw_starting_stream(jax.random.fold_in(jax.random.fold_in(seeds[12], part), 71), part),
        "multiplier_matrix": gaussian(seeds[1], (LAYERS, D, W), D ** -0.5, 0.125, ((1, 4), (2, 4))),
        "memory_path_matrix": gaussian(seeds[2], (LAYERS, D, W), D ** -0.5, 0.125, ((1, 4), (2, 4))),
        "filter_coefficients": gaussian(seeds[3], (LAYERS, CONV, W), CONV ** -0.5, 3.0, ((2, 4),)),
        "memory_valve_matrix": gaussian(seeds[4], (LAYERS, BLOCKS, BLOCK_W, BLOCK_W), BLOCK_W ** -0.5, 0.375, ((1, 4),)),
        "entry_valve_matrix": gaussian(seeds[5], (LAYERS, BLOCKS, BLOCK_W, BLOCK_W), BLOCK_W ** -0.5, 0.375, ((1, 4),)),
        "forgetting_parameters": draw_forgetting_parameters(jax.random.fold_in(seeds[12], 71), part),
        "timestep_forgetting_multiplier": draw_timestep_forgetting_multiplier(jax.random.fold_in(jax.random.fold_in(seeds[12], part), 71), part),
        "spike_extra": draw_spike_extra(jax.random.fold_in(jax.random.fold_in(seeds[12], part), 71), part),
        "exit_projector_matrix": gaussian(seeds[9], (LAYERS, W, D), W ** -0.5, 0.125, ((1, 4), (2, 4))),
        "prelude_rms_gains": jnp.clip(1.0 + 0.18 * jax.random.normal(seeds[10], (LAYERS, D), jnp.float32), 0.1, 1.9),
        "finishing_rms_gains": jnp.clip(1.0 + 0.18 * jax.random.normal(seeds[11], (D,), jnp.float32), 0.1, 1.9),
    }


EPSILON = 1e-06
SQUASH_POWER = 8.0

def norm_rows(values, gain):
    mean_square = lax.optimization_barrier(jnp.mean(values * values, axis=-1, keepdims=True))
    return values * lax.rsqrt(mean_square + EPSILON) * gain

def combine_pairs(earlier, later):
    return (earlier[0] * later[0], later[0] * earlier[1] + later[1])

def reference(starting_stream, multiplier_matrix, memory_path_matrix, filter_coefficients, memory_valve_matrix, entry_valve_matrix, forgetting_parameters, timestep_forgetting_multiplier, spike_extra, exit_projector_matrix, prelude_rms_gains, finishing_rms_gains):
    stream = starting_stream
    full_width = memory_path_matrix.shape[2]
    per_block = full_width // N_TP
    for tier_number in range(LAYERS):
        floats = stream.astype(jnp.float32)
        normed = norm_rows(floats, prelude_rms_gains[tier_number]).astype(jnp.bfloat16)
        branch = jnp.dot(normed, multiplier_matrix[tier_number], preferred_element_type=jnp.float32).astype(jnp.bfloat16)
        recurrent = jnp.dot(normed, memory_path_matrix[tier_number], preferred_element_type=jnp.float32).astype(jnp.bfloat16)
        padded = jnp.concatenate([jnp.zeros((CONV - 1, full_width), jnp.bfloat16), recurrent], axis=0)
        conv_sum = jnp.zeros((TOKENS, full_width), jnp.float32)
        for offset in range(CONV):
            conv_sum = conv_sum + padded[offset:offset + TOKENS].astype(jnp.float32) * filter_coefficients[tier_number, offset].astype(jnp.float32)
        convolved = conv_sum.astype(jnp.bfloat16)
        blocks = convolved.astype(jnp.float32).reshape(TOKENS, BLOCKS, BLOCK_W)
        memory_valve_amount = jax.nn.sigmoid(jnp.einsum('tnc,ncd->tnd', blocks, memory_valve_matrix[tier_number].astype(jnp.float32)).reshape(TOKENS, full_width))
        inject = jax.nn.sigmoid(jnp.einsum('tnc,ncd->tnd', blocks, entry_valve_matrix[tier_number].astype(jnp.float32)).reshape(TOKENS, full_width))
        logarithmic_persistence = -SQUASH_POWER * memory_valve_amount * jax.nn.softplus(-forgetting_parameters[tier_number])[None, :] * timestep_forgetting_multiplier[:, None] + spike_extra
        keep_rate = jnp.exp(logarithmic_persistence)
        driven = inject * convolved.astype(jnp.float32) * jnp.sqrt(-jnp.expm1(2.0 * logarithmic_persistence))
        state_seq = lax.associative_scan(combine_pairs, (keep_rate, driven), axis=0)[1]
        mixed_in = (jax.nn.gelu(branch.astype(jnp.float32)) * state_seq).astype(jnp.bfloat16)
        mixed_sum = jnp.zeros((TOKENS, D), jnp.float32)
        for block_no in range(N_TP):
            lower = block_no * per_block
            product = jnp.dot(mixed_in[:, lower:lower + per_block], exit_projector_matrix[tier_number, lower:lower + per_block], preferred_element_type=jnp.float32)
            mixed_sum = mixed_sum + lax.optimization_barrier(product.astype(jnp.bfloat16)).astype(jnp.float32)
        stream = (floats + mixed_sum).astype(jnp.bfloat16)
    return norm_rows(stream.astype(jnp.float32), finishing_rms_gains).astype(jnp.bfloat16)
```

```python
import functools

import jax
import jax.numpy as jnp
from jax import lax
from jax.experimental import pallas as pl
from jax.experimental.pallas import tpu as pltpu
from jax.sharding import PartitionSpec as P

BLOCK_W = 256


EPSILON = 1e-06
SQUASH_POWER = 8.0


def from_behind(value, axis, steps):
    count = lax.axis_size(axis)
    first, last = (max(0, -steps), min(count, count - steps))
    return lax.ppermute(value, axis, [(source, source + steps) for source in range(first, last)])


def entering(part, axis, combine, identity):
    place = lax.axis_index(axis)
    gathered = jax.tree.map(lambda a: lax.all_gather(a, axis), part)
    state = jax.tree.map(lambda a, e: jnp.zeros_like(a) + jnp.asarray(e, a.dtype), part, identity)

    def one(lap, state):
        return combine(
            state, jax.tree.map(lambda a: lax.dynamic_index_in_dim(a, lap, 0, False), gathered)
        )

    return lax.fori_loop(0, place, one, state)


def combine_pairs(earlier, later):
    return (earlier[0] * later[0], later[0] * earlier[1] + later[1])


def gather_rows(own_cols):
    return lax.all_gather(own_cols, "tp", axis=1, tiled=True)


def on_device(
    starting_stream,
    multiplier_matrix,
    memory_path_matrix,
    filter_coefficients,
    memory_valve_matrix,
    entry_valve_matrix,
    forgetting_parameters,
    timestep_forgetting_multiplier,
    spike_extra,
    exit_projector_matrix,
    prelude_rms_gains,
    finishing_rms_gains,
):
    tok_rows = starting_stream.shape[0]
    channels = memory_path_matrix.shape[2]
    own_cols = starting_stream
    full_rows = gather_rows(starting_stream)
    for tier_number in range(memory_path_matrix.shape[0]):
        floats = full_rows.astype(jnp.float32)
        mean_square = jnp.mean(floats * floats, axis=1, keepdims=True)
        normed = (
            floats * lax.rsqrt(mean_square + EPSILON) * prelude_rms_gains[tier_number][None, :]
        ).astype(jnp.bfloat16)
        branch_acc = jnp.dot(
            normed,
            lax.all_gather(multiplier_matrix[tier_number], "sp", axis=0, tiled=True),
            preferred_element_type=jnp.float32,
        )
        recur_acc = jnp.dot(
            normed,
            lax.all_gather(memory_path_matrix[tier_number], "sp", axis=0, tiled=True),
            preferred_element_type=jnp.float32,
        )
        branch = branch_acc.astype(jnp.bfloat16)
        recurrent = recur_acc.astype(jnp.bfloat16)
        taps_now = filter_coefficients[tier_number]
        reach_back = taps_now.shape[0] - 1
        halo_rows = from_behind(recurrent[tok_rows - reach_back :], "sp", 1)
        extended = jnp.concatenate([halo_rows, recurrent], axis=0)
        conv_sum = jnp.zeros((tok_rows, channels), jnp.float32)
        for offset in range(taps_now.shape[0]):
            conv_sum = conv_sum + extended[offset : offset + tok_rows].astype(
                jnp.float32
            ) * taps_now[offset].astype(jnp.float32)
        convolved = conv_sum.astype(jnp.bfloat16)
        blocks = convolved.reshape(tok_rows, channels // BLOCK_W, BLOCK_W)
        reset_gate = jax.nn.sigmoid(
            jnp.einsum(
                "tnc,ncd->tnd",
                blocks,
                memory_valve_matrix[tier_number],
                preferred_element_type=jnp.float32,
            ).reshape(tok_rows, channels)
        )
        inject = jax.nn.sigmoid(
            jnp.einsum(
                "tnc,ncd->tnd",
                blocks,
                entry_valve_matrix[tier_number],
                preferred_element_type=jnp.float32,
            ).reshape(tok_rows, channels)
        )
        logarithmic_persistence = (
            -SQUASH_POWER
            * reset_gate
            * jax.nn.softplus(-forgetting_parameters[tier_number])[None, :]
            * timestep_forgetting_multiplier[:, None]
            + spike_extra
        )
        keep_rate = jnp.exp(logarithmic_persistence)
        driven = (
            inject
            * convolved.astype(jnp.float32)
            * jnp.sqrt(-jnp.expm1(2.0 * logarithmic_persistence))
        )
        keep_cum, state_local = lax.associative_scan(combine_pairs, (keep_rate, driven), axis=0)
        identity = (jnp.ones((channels,), jnp.float32), jnp.zeros((channels,), jnp.float32))
        carried = entering((keep_cum[-1], state_local[-1]), "sp", combine_pairs, identity)
        state_seq = state_local + keep_cum * carried[1][None, :]
        mixed_in = (jax.nn.gelu(branch.astype(jnp.float32)) * state_seq).astype(jnp.bfloat16)
        partial_value = jnp.dot(
            mixed_in,
            lax.all_gather(exit_projector_matrix[tier_number], "sp", axis=1, tiled=True),
            preferred_element_type=jnp.float32,
        )
        mixed_sum = lax.psum_scatter(
            partial_value.astype(jnp.bfloat16), "tp", scatter_dimension=1, tiled=True
        ).astype(jnp.float32)
        own_cols = (own_cols.astype(jnp.float32) + mixed_sum).astype(jnp.bfloat16)
        if tier_number + 1 < memory_path_matrix.shape[0]:
            full_rows = gather_rows(own_cols)
    floats = own_cols.astype(jnp.float32)
    full_width = floats.shape[1] * lax.axis_size("tp")
    square_sum = lax.psum(jnp.sum(floats * floats, axis=1), "tp")
    inv_rms = lax.rsqrt(square_sum / full_width + EPSILON)
    return (floats * inv_rms[:, None] * finishing_rms_gains[None, :]).astype(jnp.bfloat16)


MESH = pl.DeviceIdType.MESH
F32, BF16 = jnp.float32, jnp.bfloat16

PARTS = 2
LENT = (1,)
WHOLE = (2, 3, 4, 5)


def one_minus_exp(u):
    series = -u * (
        1 + u / 2 * (1 + u / 3 * (1 + u / 4 * (1 + u / 5 * (1 + u / 6 * (1 + u / 7)))))
    )
    return jnp.where(u > -0.35, series, 1.0 - jnp.exp(u))


def shifted(value, steps, fill):
    rows = value.shape[0]
    if steps % 8 == 0:
        top = jnp.full((steps, value.shape[1]), fill, value.dtype)
        return jnp.concatenate([top, value[: rows - steps]], axis=0)
    at = lax.broadcasted_iota(jnp.int32, value.shape, 0)
    return jnp.where(at < steps, fill, pltpu.roll(value, steps, 0))


def fused(
    sizes,
    x_ref,
    branch_w,
    memory_w,
    exit_w,
    taps_ref,
    reset_w,
    inject_w,
    rate_ref,
    mult_ref,
    spike_ref,
    gains_ref,
    final_ref,
    out_ref,
    win,
    wout,
    agx,
    xs,
    nrm,
    ext,
    halo,
    keep_s,
    state_s,
    gel_s,
    mix_s,
    lent_out,
    lent_in,
    part,
    from_sib,
    pair,
    from_far,
    cry_out,
    cry_in,
    hacc,
    mult_s,
    sq_out,
    sq_in,
    sem_own,
    sem_w_recv,
    sem_w_send,
    sem_lend,
    sem_ag_send,
    sem_ag_recv,
    sem_rs_send,
    sem_rs_recv,
    sem_h,
    sem_c_send,
    sem_c_recv,
    sem_q_send,
    sem_q_recv,
):
    layers, n_sp, n_tp, n_grp, rows, chans, feats, depth, pieces = sizes
    chips = n_tp // 2
    count = 3 * layers
    g, s, t = lax.axis_index("grp"), lax.axis_index("sp"), lax.axis_index("tp")
    core = lax.rem(t, 2)
    chip = t // 2
    sib = chip * 2 + 1 - core
    full = n_tp * feats
    inw = 1 - 2 * (s // (n_sp // 2))
    is_end = (s == 0) | (s == n_sp - 1)
    is_mid = (s > 0) & (s < n_sp - 1)

    def at_end(body):
        pl.when(is_end)(body)

    def at_mid(body):
        pl.when(is_mid)(body)

    barrier = pltpu.get_barrier_semaphore()
    for d in range(1, n_tp):
        pl.semaphore_signal(
            barrier, inc=1, device_id={"tp": lax.rem(t + d, n_tp)}, device_id_type=MESH
        )
    for d in range(1, n_sp):
        pl.semaphore_signal(
            barrier, inc=1, device_id={"sp": lax.rem(s + d, n_sp)}, device_id_type=MESH
        )
    pl.semaphore_signal(barrier, inc=1, device_id={"grp": 1 - g}, device_id_type=MESH)
    pl.semaphore_wait(barrier, n_tp - 1 + n_sp - 1 + 1)

    IN, OUT, ACROSS = 0, 1, 2

    def target(way):
        if way == ACROSS:
            return {"grp": 1 - g}
        return {"sp": s + inw} if way == IN else {"sp": s - inw}

    def own_block(m):
        return (memory_w, branch_w, exit_w)[m % 3].at[m // 3]

    def slot(m, j):
        kind = 2 * (m // 3) + m % 3 if m % 3 < 2 else m // 3
        return (win if m % 3 < 2 else wout), (kind * n_sp + j) * 2

    def cut(ref, q):
        size = ref.shape[0] // PARTS
        return ref.at[pl.ds(q * size, size)]

    def held(m, j, half, q):
        ref, at = slot(m, j)
        return cut(ref.at[at + half], q)

    def sent(src, m, j, half, q, way):
        return pltpu.make_async_remote_copy(
            src_ref=src,
            dst_ref=held(m, j, half, q),
            send_sem=sem_w_send.at[way],
            recv_sem=sem_w_recv.at[m, j, half, q],
            device_id=target(way),
            device_id_type=MESH,
        )

    def relay(m, j, q, ways):
        src = held(m, j, g, q)
        for way in ways:
            sent(src, m, j, g, q, way).start()

    def landed(m, j, half, q):
        sent(held(m, j, half, q), m, j, half, q, ACROSS).wait_recv()

    def own(m, way, half):
        for q in range(PARTS):
            sent(cut(own_block(m).at[half], q), m, s, half, q, way).start()

    def own_in(m):
        own(m, IN, g)
        if m in WHOLE:
            at_end(lambda: own(m, IN, 1 - g))

    def keep_own(m):
        ref, at = slot(m, s)
        return pltpu.make_async_copy(own_block(m), ref.at[pl.ds(at, 2)], sem_own.at[m])

    def late():
        return chip == (s + is_end.astype(jnp.int32) * inw) // (n_tp // chips)

    def own_out(m):
        own(m, OUT, g)

    def own_out_if(m, when):
        pl.when(is_mid & (late() if when else jnp.logical_not(late())))(lambda: own_out(m))

    def end_pump(m, i):
        if m % 3 == 2:
            i = lax.rem(i - 1 + late().astype(jnp.int32), n_sp - 1) + 1
        j = s + inw * i
        for q in range(PARTS):
            landed(m, j, g, q)
            relay(m, j, q, (ACROSS,))

    def mid_pump(m, k):
        j = s + inw * (k if k else -1)
        for q in range(PARTS):
            landed(m, j, g, q)
            if k == 0:
                ways = (IN,) if m in WHOLE else (IN, ACROSS)
            else:
                ways = (ACROSS,) if m in LENT else (OUT, ACROSS)
            relay(m, j, q, ways)

    def end_do(*acts):
        def body():
            for act in acts:
                act()

        at_end(body)

    def mid_do(*acts):
        def body():
            for act in acts:
                act()

        at_mid(body)

    def E(m, i):
        return lambda: end_pump(m, i)

    def M(m, k):
        return lambda: mid_pump(m, k)

    def I(m):
        return lambda: own_in(m)

    def O(m):
        return lambda: own_out(m)

    def ready(m, j):
        for q in range(PARTS):
            landed(m, j, 1 - g, q)

    def arrived(m):
        keep_own(m).wait()
        for d in range(1, n_sp):
            ready(m, lax.rem(s + d, n_sp))

    def wait_sends(way, halves):
        view = win.at[pl.ds(0, halves)]
        pltpu.make_async_remote_copy(
            src_ref=view,
            dst_ref=view,
            send_sem=sem_w_send.at[way],
            recv_sem=sem_w_recv.at[0, 0, 0, 0],
            device_id=target(ACROSS),
            device_id_type=MESH,
        ).wait_send()

    def close_weights():
        lent, whole = len(LENT), len(WHOLE)

        @at_end
        def _():
            wait_sends(IN, count + whole)
            wait_sends(ACROSS, (count - lent) * (n_sp - 1))

        @at_mid
        def _():
            wait_sends(IN, 2 * count)
            wait_sends(OUT, (count - lent) * (n_sp - 1))
            wait_sends(ACROSS, count * (n_sp - 1) - whole)

    def ag_copy(src, layer, owner, k, where):
        return pltpu.make_async_remote_copy(
            src_ref=src,
            dst_ref=agx.at[layer, owner],
            send_sem=sem_ag_send.at[layer, k],
            recv_sem=sem_ag_recv.at[layer, owner],
            device_id={"tp": where},
            device_id_type=MESH,
        )

    def ag_start(layer, src):
        for d in range(1, chips):
            ag_copy(src, layer, t, d, lax.rem(t + 2 * d, n_tp)).start()
        ag_copy(src, layer, t, 0, sib).start()

    def ag_finish(layer, src):
        for d in range(1, chips):
            owner = lax.rem(t + 2 * d, n_tp)
            block = agx.at[layer, owner]
            ag_copy(block, layer, owner, d, sib).wait_recv()
            ag_copy(block, layer, owner, chips + d, sib).start()
        ag_copy(src, layer, sib, 0, sib).wait_recv()
        for d in range(1, chips):
            owner = lax.rem(sib + 2 * d, n_tp)
            ag_copy(agx.at[layer, owner], layer, owner, d, sib).wait_recv()

    def ag_close(layer, src):
        for d in range(1, chips):
            ag_copy(src, layer, t, d, sib).wait_send()
            ag_copy(src, layer, t, chips + d, sib).wait_send()
        ag_copy(src, layer, t, 0, sib).wait_send()

    def lend_rows():
        return pltpu.make_async_remote_copy(
            src_ref=x_ref,
            dst_ref=agx.at[layers, t],
            send_sem=sem_lend.at[0],
            recv_sem=sem_ag_recv.at[layers, t],
            device_id=target(IN),
            device_id_type=MESH,
        )

    def lend_back():
        return pltpu.make_async_remote_copy(
            src_ref=lent_out,
            dst_ref=lent_in,
            send_sem=sem_lend.at[1],
            recv_sem=sem_lend.at[2],
            device_id=target(OUT),
            device_id_type=MESH,
        )

    step = rows // pieces

    def normalize(layer, gain_row):
        def one(i, carry):
            at = pl.ds(pl.multiple_of(i * step, step), step)
            total = jnp.zeros((step, 1), F32)
            for p in range(n_tp):
                f = agx[layer, p, at].astype(F32)
                total = total + jnp.sum(f * f, axis=1, keepdims=True)
            inv = lax.rsqrt(total / full + EPSILON)
            for p in range(n_tp):
                cols = slice(p * feats, (p + 1) * feats)
                f = agx[layer, p, at].astype(F32)
                gain = gains_ref[gain_row : gain_row + 1, cols]
                nrm[at, cols] = (f * inv * gain).astype(BF16)
            return carry

        lax.fori_loop(0, pieces, one, 0)

    def project(idx):
        total = None
        for j in range(n_sp):
            at = (idx * n_sp + j) * 2
            term = jnp.dot(
                nrm[:, j * depth : (j + 1) * depth],
                win[at : at + 2].reshape(depth, chans),
                preferred_element_type=F32,
            )
            total = term if total is None else total + term
        return total.astype(BF16)

    def halo_copy(layer):
        return pltpu.make_async_remote_copy(
            src_ref=ext.at[layer, pl.ds(rows, 8)],
            dst_ref=halo.at[layer],
            send_sem=sem_h.at[layer, 0],
            recv_sem=sem_h.at[layer, 1],
            device_id={"sp": s + 1},
            device_id_type=MESH,
        )

    def carry_copy(layer, d):
        return pltpu.make_async_remote_copy(
            src_ref=cry_out.at[layer],
            dst_ref=cry_in.at[layer, s],
            send_sem=sem_c_send.at[layer, d],
            recv_sem=sem_c_recv.at[layer, s],
            device_id={"sp": s + d},
            device_id_type=MESH,
        )

    def carry_wait(layer, j):
        pltpu.make_async_remote_copy(
            src_ref=cry_out.at[layer],
            dst_ref=cry_in.at[layer, j],
            send_sem=sem_c_send.at[layer, 0],
            recv_sem=sem_c_recv.at[layer, j],
            device_id={"sp": s},
            device_id_type=MESH,
        ).wait_recv()

    def rs_copy(src, dst, layer, k, where):
        return pltpu.make_async_remote_copy(
            src_ref=src,
            dst_ref=dst,
            send_sem=sem_rs_send.at[layer, k],
            recv_sem=sem_rs_recv.at[layer, k],
            device_id={"tp": where},
            device_id_type=MESH,
        )

    def near_copy(layer, q):
        to = lax.rem(sib + 2 * q, n_tp)
        return rs_copy(part.at[layer, to], from_sib.at[layer, q], layer, q, sib)

    def far_copy(layer, q):
        where = lax.rem(t + 2 * q, n_tp)
        return rs_copy(pair.at[layer, q], from_far.at[layer, q], layer, chips + q, where)

    def send_halo(layer):
        @pl.when(s < n_sp - 1)
        def _():
            halo_copy(layer).start()

    def take_halo(layer):
        @pl.when(s == 0)
        def _():
            halo[layer] = jnp.zeros((8, chans), F32)

        @pl.when(s > 0)
        def _():
            halo_copy(layer).wait_recv()

        ext[layer, :8] = halo[layer]

    def gates(layer, b):
        n_taps = taps_ref.shape[1]
        base = 8 - (n_taps - 1)
        cols = slice(b * BLOCK_W, (b + 1) * BLOCK_W)
        conv = jnp.zeros((rows, BLOCK_W), F32)
        for k in range(n_taps):
            tap = taps_ref[layer, k : k + 1, cols].astype(F32)
            conv = conv + ext[layer, base + k : base + k + rows, cols] * tap
        conv = conv.astype(BF16)
        reset = jax.nn.sigmoid(
            jnp.dot(conv, reset_w[layer, b], preferred_element_type=F32)
        )
        inject = jax.nn.sigmoid(
            jnp.dot(conv, inject_w[layer, b], preferred_element_type=F32)
        )
        log_keep = (
            reset * rate_ref[layer : layer + 1, cols] * mult_s[...] + spike_ref[:, cols]
        )
        keep = jnp.exp(log_keep)
        state = inject * conv.astype(F32) * jnp.sqrt(one_minus_exp(2.0 * log_keep))
        lag = 1
        while lag < rows:
            state = keep * shifted(state, lag, 0.0) + state
            keep = keep * shifted(keep, lag, 1.0)
            lag *= 2
        keep_s[:, cols] = keep
        state_s[:, cols] = state
        cry_out[layer, 0:1, cols] = keep[rows - 1 :]
        cry_out[layer, 1:2, cols] = state[rows - 1 :]

    def send_carry(layer):
        for d in range(1, n_sp):

            @pl.when(s + d < n_sp)
            def _():
                carry_copy(layer, d).start()

    def take_carry(layer):
        hacc[...] = jnp.zeros((1, chans), F32)
        for j in range(n_sp - 1):

            @pl.when(j < s)
            def _():
                carry_wait(layer, j)
                hacc[...] = cry_in[layer, j, 0:1] * hacc[...] + cry_in[layer, j, 1:2]

    def mix():
        mix_s[...] = (
            gel_s[...] * (state_s[...] + keep_s[...] * hacc[...])
        ).astype(BF16)

    def chips_on(j):
        return lax.rem(j // 2 - chip + chips, chips)

    def product(layer, j):
        at = (layer * n_sp + j) * 2
        part[layer, j] = jnp.dot(
            mix_s[...],
            wout[pl.ds(at, 2)].reshape(chans, depth),
            preferred_element_type=F32,
        ).astype(BF16)

        @pl.when(lax.rem(j, 2) != core)
        def _():
            near_copy(layer, chips_on(j)).start()

    def pass_on(layer, j):
        q = chips_on(j)

        @pl.when((lax.rem(j, 2) == core) & (q != 0))
        def _():
            near_copy(layer, q).wait_recv()
            pair[layer, q] = (
                part[layer, j].astype(F32) + from_sib[layer, q].astype(F32)
            ).astype(BF16)
            far_copy(layer, q).start()

    def exit_order(i):
        turned = lax.rem(i - 1 + late().astype(jnp.int32), n_sp - 1) + 1
        end_step = turned
        mid_step = (-1, 1, 2)[i - 1]
        e = is_end.astype(jnp.int32)
        return s + inw * (e * end_step + (1 - e) * mid_step)

    def project_out(layer, ahead):
        m = 3 * layer + 2
        keep_own(m).wait()
        product(layer, s)
        before = s
        for i in range(1, n_sp):
            ahead(i)
            j = exit_order(i)
            ready(m, j)
            product(layer, j)
            pass_on(layer, before)
            before = j
        pass_on(layer, before)

    def close_layer(layer, src):
        near_copy(layer, 0).wait_recv()
        mixed = part[layer, t].astype(F32) + from_sib[layer, 0].astype(F32)
        for q in range(1, chips):
            far_copy(layer, q).wait_recv()
            mixed = mixed + from_far[layer, q].astype(F32)
        fresh = (src[...].astype(F32) + mixed).astype(BF16)
        xs[layer + 1] = fresh

    ag_start(0, x_ref)
    own_in(0)
    at_end(lambda: lend_rows().start())
    own_in(1)
    mid_do(O(0), O(3))
    for m in range(count):
        keep_own(m).start()
    agx[0, t] = x_ref[...]
    mult_s[...] = jnp.broadcast_to(mult_ref[...], (128, rows)).T[:, 0:1]

    end_do(E(0, 1), I(2))
    mid_do(M(0, 0), M(0, 1))
    ag_finish(0, x_ref)
    normalize(0, 0)

    @at_mid
    def _():
        lend_rows().wait_recv()
        ag_start(layers, agx.at[layers, t])

    mid_do(M(0, 2), I(2), M(1, 1))
    end_do(E(3, 1), E(0, 2), E(0, 3), I(3))
    arrived(0)
    ext[0, 8:] = project(0).astype(F32)
    send_halo(0)
    mid_do(M(1, 0), O(4))
    take_halo(0)
    gates(0, 0)
    mid_do(M(1, 2), I(3))
    gates(0, 1)
    send_carry(0)
    end_do(E(4, 1), I(4))

    @at_mid
    def _():
        arrived(1)
        gel_s[...] = jax.nn.gelu(project(1).astype(F32))
        ag_finish(layers, agx.at[layers, t])
        normalize(layers, 0)
        lent_out[...] = project(1)
        lend_back().start()
        own_out_if(2, False)

    mid_do(M(2, 0), M(2, 1))

    @at_end
    def _():
        keep_own(1).wait()
        lend_back().wait_recv()
        gel_s[...] = jax.nn.gelu(lent_in[...].astype(F32))

    take_carry(0)
    mix()

    def ahead(i):
        if i == 1:
            end_do(E(2, 1), I(5))
        elif i == 2:
            end_do(E(2, 2))
        else:
            end_do(E(2, 3))
            mid_do(M(2, 2), lambda: own_out_if(2, True), I(4), M(3, 1), M(3, 0))

    project_out(0, ahead)
    close_layer(0, x_ref)

    ag_start(1, xs.at[1])
    agx[1, t] = xs[1]
    mid_do(M(3, 2), I(5))
    end_do(E(3, 2), E(3, 3))
    ag_finish(1, xs.at[1])
    normalize(1, 1)
    arrived(3)
    ext[1, 8:] = project(2).astype(F32)
    send_halo(1)
    mid_do(M(4, 1), M(4, 0))
    take_halo(1)
    gates(1, 0)
    mid_do(M(4, 2), lambda: own_out_if(5, False))
    end_do(E(4, 2))
    gates(1, 1)
    send_carry(1)
    mid_do(M(5, 1), M(5, 0), M(5, 2), lambda: own_out_if(5, True))
    end_do(E(4, 3))
    arrived(4)
    gel_s[...] = jax.nn.gelu(project(3).astype(F32))
    take_carry(1)
    mix()

    def ahead_last(i):
        end_do(E(5, i))

    project_out(1, ahead_last)
    close_layer(1, xs.at[1])

    fresh = xs[layers].astype(F32)
    square = jnp.sum(fresh * fresh, axis=1, keepdims=True)
    sq_out[...] = jnp.broadcast_to(square, (rows, 128)).T[0:8]

    def sq_copy(d):
        return pltpu.make_async_remote_copy(
            src_ref=sq_out,
            dst_ref=sq_in.at[d],
            send_sem=sem_q_send.at[d],
            recv_sem=sem_q_recv.at[d],
            device_id={"tp": lax.rem(t + d, n_tp)},
            device_id_type=MESH,
        )

    for d in range(1, n_tp):
        sq_copy(d).start()
    total = sq_out[0:1]
    for d in range(1, n_tp):
        sq_copy(d).wait_recv()
        total = total + sq_in[d, 0:1]
    inv = lax.rsqrt(total / full + EPSILON)
    inv = jnp.broadcast_to(inv, (128, rows)).T[:, 0:1]
    out_ref[...] = (xs[layers].astype(F32) * inv * final_ref[...]).astype(BF16)

    close_weights()
    at_end(lambda: lend_rows().wait_send())

    @at_mid
    def _():
        ag_close(layers, agx.at[layers, t])
        lend_back().wait_send()

    for layer in range(layers):
        ag_close(layer, x_ref if layer == 0 else xs.at[layer])

        @pl.when(s < n_sp - 1)
        def _():
            halo_copy(layer).wait_send()

        for d in range(1, n_sp):

            @pl.when(s + d < n_sp)
            def _():
                carry_copy(layer, d).wait_send()

        for q in range(chips):
            near_copy(layer, q).wait_send()
        for q in range(1, chips):
            far_copy(layer, q).wait_send()
    for d in range(1, n_tp):
        sq_copy(d).wait_send()


def in_one_kernel(
    sizes_of,
    starting_stream,
    multiplier_matrix,
    memory_path_matrix,
    filter_coefficients,
    memory_valve_matrix,
    entry_valve_matrix,
    forgetting_parameters,
    timestep_forgetting_multiplier,
    spike_extra,
    exit_projector_matrix,
    prelude_rms_gains,
    finishing_rms_gains,
):
    n_grp, n_sp, n_tp = sizes_of
    rows, feats = starting_stream.shape
    layers, depth, chans = memory_path_matrix.shape
    pieces = rows // 128 if rows % 128 == 0 else 1
    sizes = (layers, n_sp, n_tp, n_grp, rows, chans, feats, depth, pieces)
    chips = n_tp // 2
    half_in = (layers, 2, depth // 2, chans)
    half_out = (layers, 2, chans // 2, depth)
    rate = -SQUASH_POWER * jax.nn.softplus(-forgetting_parameters)
    vmem = pl.BlockSpec(memory_space=pltpu.VMEM)
    hbm = pl.BlockSpec(memory_space=pl.ANY)
    count = 3 * layers
    dma = pltpu.SemaphoreType.DMA
    return pl.pallas_call(
        functools.partial(fused, sizes),
        out_shape=jax.ShapeDtypeStruct((rows, feats), BF16),
        in_specs=[vmem, hbm, hbm, hbm] + [vmem] * 8,
        out_specs=vmem,
        scratch_shapes=[
            pltpu.VMEM((2 * layers * n_sp * 2, depth // 2, chans), BF16),
            pltpu.VMEM((layers * n_sp * 2, chans // 2, depth), BF16),
            pltpu.VMEM((layers + 1, n_tp, rows, feats), BF16),
            pltpu.VMEM((layers + 1, rows, feats), BF16),
            pltpu.VMEM((rows, n_tp * feats), BF16),
            pltpu.VMEM((layers, 8 + rows, chans), F32),
            pltpu.VMEM((layers, 8, chans), F32),
            pltpu.VMEM((rows, chans), F32),
            pltpu.VMEM((rows, chans), F32),
            pltpu.VMEM((rows, chans), F32),
            pltpu.VMEM((rows, chans), BF16),
            pltpu.VMEM((rows, chans), BF16),
            pltpu.VMEM((rows, chans), BF16),
            pltpu.VMEM((layers, n_tp, rows, feats), BF16),
            pltpu.VMEM((layers, chips, rows, feats), BF16),
            pltpu.VMEM((layers, chips, rows, feats), BF16),
            pltpu.VMEM((layers, chips, rows, feats), BF16),
            pltpu.VMEM((layers, 2, chans), F32),
            pltpu.VMEM((layers, n_sp, 2, chans), F32),
            pltpu.VMEM((1, chans), F32),
            pltpu.VMEM((rows, 1), F32),
            pltpu.VMEM((8, rows), F32),
            pltpu.VMEM((n_tp, 8, rows), F32),
            dma((count,)),
            dma((count, n_sp, 2, PARTS)),
            dma((3,)),
            dma((3,)),
            dma((layers + 1, 2 * chips)),
            dma((layers + 1, n_tp)),
            dma((layers, 2 * chips)),
            dma((layers, 2 * chips)),
            dma((layers, 2)),
            dma((layers, n_sp)),
            dma((layers, n_sp)),
            dma((n_tp,)),
            dma((n_tp,)),
        ],
        compiler_params=pltpu.CompilerParams(
            collective_id=0, has_side_effects=True, vmem_limit_bytes=60 * 2**20
        ),
    )(
        starting_stream,
        multiplier_matrix.reshape(half_in),
        memory_path_matrix.reshape(half_in),
        exit_projector_matrix.reshape(half_out),
        filter_coefficients,
        memory_valve_matrix,
        entry_valve_matrix,
        rate,
        timestep_forgetting_multiplier.reshape(1, rows),
        spike_extra,
        prelude_rms_gains,
        finishing_rms_gains.reshape(1, feats),
    )


def on_each(sizes_of, *arrays):
    stream, memory = arrays[0], arrays[2]
    n_grp, n_sp, n_tp = sizes_of
    rows, feats = stream.shape
    depth, chans = memory.shape[1:]
    fits = (
        n_grp == 2
        and n_sp == 4
        and memory.shape[0] == 2
        and n_tp % 2 == 0
        and rows % 128 == 0
        and depth % 128 == 0
        and feats % 128 == 0
        and chans % BLOCK_W == 0
        and depth == feats
        and n_sp == n_tp
    )
    if fits:
        return in_one_kernel(sizes_of, *arrays)
    return on_device(*arrays)


def solution(mesh):
    sizes_of = tuple(mesh.shape[axis] for axis in ("grp", "sp", "tp"))
    body = functools.partial(on_each, sizes_of)
    return jax.shard_map(
        body,
        mesh=mesh,
        in_specs=(
            P(("grp", "sp"), "tp"),
            P(None, "sp", "tp"),
            P(None, "sp", "tp"),
            P(None, None, "tp"),
            P(None, "tp", None, None),
            P(None, "tp", None, None),
            P(None, "tp"),
            P(("grp", "sp")),
            P(("grp", "sp"), "tp"),
            P(None, "tp", "sp"),
            P(),
            P("tp"),
        ),
        out_specs=P(("grp", "sp"), "tp"),
        check_vma=False,
    )
```

```python
import functools

import jax
import jax.numpy as jnp
from jax import lax
from jax.experimental import pallas as pl
from jax.experimental.pallas import tpu as pltpu
from jax.sharding import PartitionSpec as P

BLOCK_W = 256


EPSILON = 1e-06
SQUASH_POWER = 8.0


def from_behind(value, axis, steps):
    count = lax.axis_size(axis)
    first, last = (max(0, -steps), min(count, count - steps))
    return lax.ppermute(value, axis, [(source, source + steps) for source in range(first, last)])


def entering(part, axis, combine, identity):
    place = lax.axis_index(axis)
    gathered = jax.tree.map(lambda a: lax.all_gather(a, axis), part)
    state = jax.tree.map(lambda a, e: jnp.zeros_like(a) + jnp.asarray(e, a.dtype), part, identity)

    def one(lap, state):
        return combine(
            state, jax.tree.map(lambda a: lax.dynamic_index_in_dim(a, lap, 0, False), gathered)
        )

    return lax.fori_loop(0, place, one, state)


def combine_pairs(earlier, later):
    return (earlier[0] * later[0], later[0] * earlier[1] + later[1])


def gather_rows(own_cols):
    return lax.all_gather(own_cols, "tp", axis=1, tiled=True)


def on_device(
    starting_stream,
    multiplier_matrix,
    memory_path_matrix,
    filter_coefficients,
    memory_valve_matrix,
    entry_valve_matrix,
    forgetting_parameters,
    timestep_forgetting_multiplier,
    spike_extra,
    exit_projector_matrix,
    prelude_rms_gains,
    finishing_rms_gains,
):
    tok_rows = starting_stream.shape[0]
    channels = memory_path_matrix.shape[2]
    own_cols = starting_stream
    full_rows = gather_rows(starting_stream)
    for tier_number in range(memory_path_matrix.shape[0]):
        floats = full_rows.astype(jnp.float32)
        mean_square = jnp.mean(floats * floats, axis=1, keepdims=True)
        normed = (
            floats * lax.rsqrt(mean_square + EPSILON) * prelude_rms_gains[tier_number][None, :]
        ).astype(jnp.bfloat16)
        branch_acc = jnp.dot(
            normed,
            lax.all_gather(multiplier_matrix[tier_number], "sp", axis=0, tiled=True),
            preferred_element_type=jnp.float32,
        )
        recur_acc = jnp.dot(
            normed,
            lax.all_gather(memory_path_matrix[tier_number], "sp", axis=0, tiled=True),
            preferred_element_type=jnp.float32,
        )
        branch = branch_acc.astype(jnp.bfloat16)
        recurrent = recur_acc.astype(jnp.bfloat16)
        taps_now = filter_coefficients[tier_number]
        reach_back = taps_now.shape[0] - 1
        halo_rows = from_behind(recurrent[tok_rows - reach_back :], "sp", 1)
        extended = jnp.concatenate([halo_rows, recurrent], axis=0)
        conv_sum = jnp.zeros((tok_rows, channels), jnp.float32)
        for offset in range(taps_now.shape[0]):
            conv_sum = conv_sum + extended[offset : offset + tok_rows].astype(
                jnp.float32
            ) * taps_now[offset].astype(jnp.float32)
        convolved = conv_sum.astype(jnp.bfloat16)
        blocks = convolved.reshape(tok_rows, channels // BLOCK_W, BLOCK_W)
        reset_gate = jax.nn.sigmoid(
            jnp.einsum(
                "tnc,ncd->tnd",
                blocks,
                memory_valve_matrix[tier_number],
                preferred_element_type=jnp.float32,
            ).reshape(tok_rows, channels)
        )
        inject = jax.nn.sigmoid(
            jnp.einsum(
                "tnc,ncd->tnd",
                blocks,
                entry_valve_matrix[tier_number],
                preferred_element_type=jnp.float32,
            ).reshape(tok_rows, channels)
        )
        logarithmic_persistence = (
            -SQUASH_POWER
            * reset_gate
            * jax.nn.softplus(-forgetting_parameters[tier_number])[None, :]
            * timestep_forgetting_multiplier[:, None]
            + spike_extra
        )
        keep_rate = jnp.exp(logarithmic_persistence)
        driven = (
            inject
            * convolved.astype(jnp.float32)
            * jnp.sqrt(-jnp.expm1(2.0 * logarithmic_persistence))
        )
        keep_cum, state_local = lax.associative_scan(combine_pairs, (keep_rate, driven), axis=0)
        identity = (jnp.ones((channels,), jnp.float32), jnp.zeros((channels,), jnp.float32))
        carried = entering((keep_cum[-1], state_local[-1]), "sp", combine_pairs, identity)
        state_seq = state_local + keep_cum * carried[1][None, :]
        mixed_in = (jax.nn.gelu(branch.astype(jnp.float32)) * state_seq).astype(jnp.bfloat16)
        partial_value = jnp.dot(
            mixed_in,
            lax.all_gather(exit_projector_matrix[tier_number], "sp", axis=1, tiled=True),
            preferred_element_type=jnp.float32,
        )
        mixed_sum = lax.psum_scatter(
            partial_value.astype(jnp.bfloat16), "tp", scatter_dimension=1, tiled=True
        ).astype(jnp.float32)
        own_cols = (own_cols.astype(jnp.float32) + mixed_sum).astype(jnp.bfloat16)
        if tier_number + 1 < memory_path_matrix.shape[0]:
            full_rows = gather_rows(own_cols)
    floats = own_cols.astype(jnp.float32)
    full_width = floats.shape[1] * lax.axis_size("tp")
    square_sum = lax.psum(jnp.sum(floats * floats, axis=1), "tp")
    inv_rms = lax.rsqrt(square_sum / full_width + EPSILON)
    return (floats * inv_rms[:, None] * finishing_rms_gains[None, :]).astype(jnp.bfloat16)


MESH = pl.DeviceIdType.MESH
F32, BF16 = jnp.float32, jnp.bfloat16

PARTS = 4
BANDS = 2
LENT = (0, 1)
WHOLE = (1, 2, 3, 4, 5)


def one_minus_exp(u):
    series = -u * (
        1 + u / 2 * (1 + u / 3 * (1 + u / 4 * (1 + u / 5 * (1 + u / 6 * (1 + u / 7)))))
    )
    return jnp.where(u > -0.35, series, 1.0 - jnp.exp(u))


def shifted(value, steps, fill):
    rows = value.shape[0]
    if steps % 8 == 0:
        top = jnp.full((steps, value.shape[1]), fill, value.dtype)
        return jnp.concatenate([top, value[: rows - steps]], axis=0)
    at = lax.broadcasted_iota(jnp.int32, value.shape, 0)
    return jnp.where(at < steps, fill, pltpu.roll(value, steps, 0))


def fused(
    sizes,
    x_ref,
    branch_w,
    memory_w,
    exit_w,
    taps_ref,
    reset_w,
    inject_w,
    rate_ref,
    mult_ref,
    spike_ref,
    gains_ref,
    final_ref,
    out_ref,
    win,
    wout,
    agx,
    xs,
    nrm,
    nrm_lent,
    ext,
    halo,
    keep_s,
    state_s,
    gel_s,
    mix_s,
    lent_out,
    lent_in,
    part,
    from_sib,
    pair,
    from_far,
    cry_out,
    cry_in,
    hacc,
    mult_s,
    sq_out,
    sq_in,
    sem_own,
    sem_w_recv,
    sem_w_send,
    sem_lend,
    sem_ag_send,
    sem_ag_recv,
    sem_rs_send,
    sem_rs_recv,
    sem_h,
    sem_c_send,
    sem_c_recv,
    sem_q_send,
    sem_q_recv,
):
    layers, n_sp, n_tp, n_grp, rows, chans, feats, depth, pieces = sizes
    chips = n_tp // 2
    count = 3 * layers
    g, s, t = lax.axis_index("grp"), lax.axis_index("sp"), lax.axis_index("tp")
    core = lax.rem(t, 2)
    chip = t // 2
    sib = chip * 2 + 1 - core
    full = n_tp * feats
    inw = 1 - 2 * (s // (n_sp // 2))
    is_end = (s == 0) | (s == n_sp - 1)
    is_mid = (s > 0) & (s < n_sp - 1)

    def at_end(body):
        pl.when(is_end)(body)

    def at_mid(body):
        pl.when(is_mid)(body)

    barrier = pltpu.get_barrier_semaphore()
    for d in range(1, n_tp):
        pl.semaphore_signal(
            barrier, inc=1, device_id={"tp": lax.rem(t + d, n_tp)}, device_id_type=MESH
        )
    for d in range(1, n_sp):
        pl.semaphore_signal(
            barrier, inc=1, device_id={"sp": lax.rem(s + d, n_sp)}, device_id_type=MESH
        )
    pl.semaphore_signal(barrier, inc=1, device_id={"grp": 1 - g}, device_id_type=MESH)
    pl.semaphore_wait(barrier, n_tp - 1 + n_sp - 1 + 1)

    IN, OUT, ACROSS = 0, 1, 2

    def target(way):
        if way == ACROSS:
            return {"grp": 1 - g}
        return {"sp": s + inw} if way == IN else {"sp": s - inw}

    def own_block(m):
        return (memory_w, branch_w, exit_w)[m % 3].at[m // 3]

    def slot(m, j):
        kind = 2 * (m // 3) + m % 3 if m % 3 < 2 else m // 3
        return (win if m % 3 < 2 else wout), (kind * n_sp + j) * 2

    def cut(ref, q):
        size = ref.shape[0] // PARTS
        return ref.at[pl.ds(q * size, size)]

    def held(m, j, half, q):
        ref, at = slot(m, j)
        return cut(ref.at[at + half], q)

    def sent(src, m, j, half, q, way):
        return pltpu.make_async_remote_copy(
            src_ref=src,
            dst_ref=held(m, j, half, q),
            send_sem=sem_w_send.at[way],
            recv_sem=sem_w_recv.at[m, j, half, q],
            device_id=target(way),
            device_id_type=MESH,
        )

    def relay(m, j, q, ways):
        src = held(m, j, g, q)
        for way in ways:
            sent(src, m, j, g, q, way).start()

    def landed(m, j, half, q):
        sent(held(m, j, half, q), m, j, half, q, ACROSS).wait_recv()

    def own(m, way, half, q):
        sent(cut(own_block(m).at[half], q), m, s, half, q, way).start()

    def own_both(m, way):
        for q in range(PARTS):
            own(m, way, g, q)

    halves = [(1, g)]
    for m in range(2, count):
        halves += [(m, g), (m - 1, 1 - g)]
    halves.append((count - 1, 1 - g))
    end_line = [(m, half, q) for m, half in halves for q in range(PARTS)]
    mid_in_line = [(m, q) for m in range(1, count) for q in range(PARTS)]
    def feed_end(steps):
        steps *= PARTS // 2
        for m, half, q in end_line[:steps]:
            own(m, IN, half, q)
        del end_line[:steps]

    def feed_in(steps):
        for m, q in mid_in_line[:steps]:
            own(m, IN, g, q)
        del mid_in_line[:steps]

    def keep_own(m):
        ref, at = slot(m, s)
        return pltpu.make_async_copy(own_block(m), ref.at[pl.ds(at, 2)], sem_own.at[m])

    def late():
        return chip == (s + is_end.astype(jnp.int32) * inw) // (n_tp // chips)

    def end_turn(i):
        return lax.rem(i - 1 + late().astype(jnp.int32), n_sp - 1) + 1

    def own_out_if(m, when):
        @pl.when(late() if when else jnp.logical_not(late()))
        def _():
            own_both(m, OUT)

    def end_pump(m, i, feed):
        j = s + inw * (end_turn(i) if m == count - 1 else i)
        for q in range(PARTS):
            landed(m, j, g, q)
            relay(m, j, q, (ACROSS,))
            if q % (PARTS // 2) == PARTS // 2 - 1:
                feed_end(feed)

    def mid_pump(m, k, feed):
        j = s + inw * (k if k else -1)
        for q in range(PARTS):
            landed(m, j, g, q)
            if k == 0:
                ways = (IN,) if m in WHOLE else (IN, ACROSS)
            else:
                ways = (ACROSS,) if m in LENT else (OUT, ACROSS)
            relay(m, j, q, ways)
        feed_in(feed)

    def end_do(*acts):
        def body():
            for act in acts:
                act()

        at_end(body)

    def mid_do(*acts):
        def body():
            for act in acts:
                act()

        at_mid(body)

    def E(m, i, feed=0):
        return lambda: end_pump(m, i, feed)

    def M(m, k, feed=0):
        return lambda: mid_pump(m, k, feed)

    def F(steps):
        return lambda: feed_end(steps)

    def ready(m, j):
        for q in range(PARTS):
            landed(m, j, 1 - g, q)

    def arrived(m):
        keep_own(m).wait()
        for d in range(1, n_sp):
            ready(m, lax.rem(s + d, n_sp))

    def wait_sends(way, halves):
        view = win.at[pl.ds(0, halves)]
        pltpu.make_async_remote_copy(
            src_ref=view,
            dst_ref=view,
            send_sem=sem_w_send.at[way],
            recv_sem=sem_w_recv.at[0, 0, 0, 0],
            device_id=target(ACROSS),
            device_id_type=MESH,
        ).wait_send()

    def close_weights():
        lent, whole = len(LENT), len(WHOLE)

        @at_end
        def _():
            wait_sends(IN, count + whole)
            wait_sends(ACROSS, (count - lent) * (n_sp - 1))

        @at_mid
        def _():
            wait_sends(IN, 2 * count)
            wait_sends(OUT, (count - lent) * (n_sp - 1))
            wait_sends(ACROSS, count * (n_sp - 1) - whole)

    def band(ref, h):
        return ref.at[pl.ds(h * (rows // BANDS), rows // BANDS)]

    def ag_copy(src, layer, owner, k, h, where):
        return pltpu.make_async_remote_copy(
            src_ref=band(src, h),
            dst_ref=band(agx.at[layer, owner], h),
            send_sem=sem_ag_send.at[layer, k, h],
            recv_sem=sem_ag_recv.at[layer, owner, h],
            device_id={"tp": where},
            device_id_type=MESH,
        )

    def ag_start(layer, src, h):
        for d in range(1, chips):
            ag_copy(src, layer, t, d, h, lax.rem(t + 2 * d, n_tp)).start()
        ag_copy(src, layer, t, 0, h, sib).start()

    def ag_finish(layer, src):
        for h in range(BANDS):
            for d in range(1, chips):
                owner = lax.rem(t + 2 * d, n_tp)
                block = agx.at[layer, owner]
                ag_copy(block, layer, owner, d, h, sib).wait_recv()
                ag_copy(block, layer, owner, chips + d, h, sib).start()
        for h in range(BANDS):
            ag_copy(src, layer, sib, 0, h, sib).wait_recv()
            for d in range(1, chips):
                owner = lax.rem(sib + 2 * d, n_tp)
                ag_copy(agx.at[layer, owner], layer, owner, d, h, sib).wait_recv()

    def ag_close(layer, src):
        for h in range(BANDS):
            for d in range(1, chips):
                ag_copy(src, layer, t, d, h, sib).wait_send()
                ag_copy(src, layer, t, chips + d, h, sib).wait_send()
            ag_copy(src, layer, t, 0, h, sib).wait_send()

    def lend_rows(h):
        return pltpu.make_async_remote_copy(
            src_ref=band(x_ref, h),
            dst_ref=band(agx.at[layers, t], h),
            send_sem=sem_lend.at[h],
            recv_sem=sem_ag_recv.at[layers, t, h],
            device_id=target(IN),
            device_id_type=MESH,
        )

    def lend_back(i):
        return pltpu.make_async_remote_copy(
            src_ref=lent_out.at[i],
            dst_ref=lent_in.at[i],
            send_sem=sem_lend.at[BANDS + i],
            recv_sem=sem_lend.at[BANDS + len(LENT) + i],
            device_id=target(OUT),
            device_id_type=MESH,
        )

    step = rows // pieces

    def normalize(layer, gain_row, nrm):
        def one(i, carry):
            at = pl.ds(pl.multiple_of(i * step, step), step)
            total = jnp.zeros((step, 1), F32)
            for p in range(n_tp):
                f = agx[layer, p, at].astype(F32)
                total = total + jnp.sum(f * f, axis=1, keepdims=True)
            inv = lax.rsqrt(total / full + EPSILON)
            for p in range(n_tp):
                cols = slice(p * feats, (p + 1) * feats)
                f = agx[layer, p, at].astype(F32)
                gain = gains_ref[gain_row : gain_row + 1, cols]
                nrm[at, cols] = (f * inv * gain).astype(BF16)
            return carry

        lax.fori_loop(0, pieces, one, 0)

    def project(idx, nrm):
        total = None
        for j in range(n_sp):
            at = (idx * n_sp + j) * 2
            term = jnp.dot(
                nrm[:, j * depth : (j + 1) * depth],
                win[at : at + 2].reshape(depth, chans),
                preferred_element_type=F32,
            )
            total = term if total is None else total + term
        return total.astype(BF16)

    def halo_copy(layer):
        return pltpu.make_async_remote_copy(
            src_ref=ext.at[layer, pl.ds(rows, 8)],
            dst_ref=halo.at[layer],
            send_sem=sem_h.at[layer, 0],
            recv_sem=sem_h.at[layer, 1],
            device_id={"sp": s + 1},
            device_id_type=MESH,
        )

    def carry_copy(layer, d):
        return pltpu.make_async_remote_copy(
            src_ref=cry_out.at[layer],
            dst_ref=cry_in.at[layer, s],
            send_sem=sem_c_send.at[layer, d],
            recv_sem=sem_c_recv.at[layer, s],
            device_id={"sp": s + d},
            device_id_type=MESH,
        )

    def carry_wait(layer, j):
        pltpu.make_async_remote_copy(
            src_ref=cry_out.at[layer],
            dst_ref=cry_in.at[layer, j],
            send_sem=sem_c_send.at[layer, 0],
            recv_sem=sem_c_recv.at[layer, j],
            device_id={"sp": s},
            device_id_type=MESH,
        ).wait_recv()

    def rs_copy(src, dst, layer, k, h, where):
        return pltpu.make_async_remote_copy(
            src_ref=src,
            dst_ref=dst,
            send_sem=sem_rs_send.at[layer, k, h],
            recv_sem=sem_rs_recv.at[layer, k, h],
            device_id={"tp": where},
            device_id_type=MESH,
        )

    def near_copy(layer, q, h):
        to = lax.rem(sib + 2 * q, n_tp)
        src, dst = band(part.at[layer, to], h), band(from_sib.at[layer, q], h)
        return rs_copy(src, dst, layer, q, h, sib)

    def far_copy(layer, q, h):
        where = lax.rem(t + 2 * q, n_tp)
        src, dst = band(pair.at[layer, q], h), band(from_far.at[layer, q], h)
        return rs_copy(src, dst, layer, chips + q, h, where)

    def first_sender(layer):
        return 1 if layer == 0 else 0

    def send_halo(layer):
        @pl.when((s >= first_sender(layer)) & (s < n_sp - 1))
        def _():
            halo_copy(layer).start()

    def take_halo(layer):
        @pl.when(s == 0)
        def _():
            halo[layer] = jnp.zeros((8, chans), F32)

        if layer == 0:

            @pl.when(s == 1)
            def _():
                halo[layer] = lent_out[0].astype(F32)[rows - 8 :]

        @pl.when(s > first_sender(layer))
        def _():
            halo_copy(layer).wait_recv()

        ext[layer, :8] = halo[layer]

    def gates(layer, b):
        n_taps = taps_ref.shape[1]
        base = 8 - (n_taps - 1)
        cols = slice(b * BLOCK_W, (b + 1) * BLOCK_W)
        conv = jnp.zeros((rows, BLOCK_W), F32)
        for k in range(n_taps):
            tap = taps_ref[layer, k : k + 1, cols].astype(F32)
            conv = conv + ext[layer, base + k : base + k + rows, cols] * tap
        conv = conv.astype(BF16)
        reset = jax.nn.sigmoid(
            jnp.dot(conv, reset_w[layer, b], preferred_element_type=F32)
        )
        inject = jax.nn.sigmoid(
            jnp.dot(conv, inject_w[layer, b], preferred_element_type=F32)
        )
        log_keep = (
            reset * rate_ref[layer : layer + 1, cols] * mult_s[...] + spike_ref[:, cols]
        )
        keep = jnp.exp(log_keep)
        state = inject * conv.astype(F32) * jnp.sqrt(one_minus_exp(2.0 * log_keep))
        lag = 1
        while lag < rows:
            state = keep * shifted(state, lag, 0.0) + state
            keep = keep * shifted(keep, lag, 1.0)
            lag *= 2
        keep_s[:, cols] = keep
        state_s[:, cols] = state
        cry_out[layer, 0:1, cols] = keep[rows - 1 :]
        cry_out[layer, 1:2, cols] = state[rows - 1 :]

    def send_carry(layer):
        for d in range(1, n_sp):

            @pl.when(s + d < n_sp)
            def _():
                carry_copy(layer, d).start()

    def take_carry(layer):
        hacc[...] = jnp.zeros((1, chans), F32)
        for j in range(n_sp - 1):

            @pl.when(j < s)
            def _():
                carry_wait(layer, j)
                hacc[...] = cry_in[layer, j, 0:1] * hacc[...] + cry_in[layer, j, 1:2]

    def mix():
        mix_s[...] = (
            gel_s[...] * (state_s[...] + keep_s[...] * hacc[...])
        ).astype(BF16)

    def chips_on(j):
        return lax.rem(j // 2 - chip + chips, chips)

    def product(layer, j):
        at = (layer * n_sp + j) * 2
        part[layer, j] = jnp.dot(
            mix_s[...],
            wout[pl.ds(at, 2)].reshape(chans, depth),
            preferred_element_type=F32,
        ).astype(BF16)

        @pl.when(lax.rem(j, 2) != core)
        def _():
            for h in range(BANDS):
                near_copy(layer, chips_on(j), h).start()

    def pass_on(layer, j):
        q = chips_on(j)

        @pl.when((lax.rem(j, 2) == core) & (q != 0))
        def _():
            for h in range(BANDS):
                at = pl.ds(h * (rows // BANDS), rows // BANDS)
                near_copy(layer, q, h).wait_recv()
                pair[layer, q, at] = (
                    part[layer, j, at].astype(F32) + from_sib[layer, q, at].astype(F32)
                ).astype(BF16)
                far_copy(layer, q, h).start()

    def exit_order(layer, i):
        end_step = end_turn(i) if layer == layers - 1 else i
        mid_step = (-1, 1, 2)[i - 1]
        e = is_end.astype(jnp.int32)
        return s + inw * (e * end_step + (1 - e) * mid_step)

    def project_out(layer, ahead):
        m = 3 * layer + 2
        keep_own(m).wait()
        product(layer, s)
        before = s
        for i in range(1, n_sp):
            ahead(i)
            j = exit_order(layer, i)
            ready(m, j)
            product(layer, j)
            pass_on(layer, before)
            before = j
        pass_on(layer, before)

    def close_layer(layer, src):
        for h in range(BANDS):
            at = pl.ds(h * (rows // BANDS), rows // BANDS)
            near_copy(layer, 0, h).wait_recv()
            mixed = part[layer, t, at].astype(F32) + from_sib[layer, 0, at].astype(F32)
            for q in range(1, chips):
                far_copy(layer, q, h).wait_recv()
                mixed = mixed + from_far[layer, q, at].astype(F32)
            xs[layer + 1, at] = (src[at].astype(F32) + mixed).astype(BF16)
            if layer + 1 < layers:
                ag_start(layer + 1, xs.at[layer + 1], h)

    own_both(0, IN)

    @at_end
    def _():
        for h in range(BANDS):
            lend_rows(h).start()
        feed_end(2)

    @at_mid
    def _():
        for h in range(BANDS):
            ag_start(0, x_ref, h)
        for m in (2, 3, 4):
            own_both(m, OUT)
        for m in LENT:
            keep_own(m).start()
        agx[0, t] = x_ref[...]

    for m in range(len(LENT), count):
        keep_own(m).start()
    mult_s[...] = jnp.broadcast_to(mult_ref[...], (128, rows)).T[:, 0:1]

    @at_mid
    def _():
        mid_pump(0, 0, PARTS)
        mid_pump(0, 1, 0)
        ag_finish(0, x_ref)
        normalize(0, 0, nrm)
        lend_rows(0).wait_recv()
        ag_start(layers, agx.at[layers, t], 0)
        mid_pump(0, 2, PARTS)
        for h in range(1, BANDS):
            lend_rows(h).wait_recv()
            ag_start(layers, agx.at[layers, t], h)
        mid_pump(1, 1, 0)
        mid_pump(1, 0, 0)
        arrived(0)
        ext[0, 8:] = project(0, nrm).astype(F32)
        send_halo(0)
        mid_pump(2, 1, 0)
        ag_finish(layers, agx.at[layers, t])
        normalize(layers, 0, nrm_lent)
        lent_out[0] = project(0, nrm_lent)
        lend_back(0).start()
        mid_pump(2, 0, PARTS)
        mid_pump(1, 2, 0)

    @at_end
    def _():
        end_pump(2, 1, 0)
        end_pump(3, 1, 0)
        end_pump(4, 1, 1)
        feed_end(2)
        end_pump(2, 2, 1)
        feed_end(2)
        lend_back(0).wait_recv()
        ext[0, 8:] = lent_in[0].astype(F32)

    take_halo(0)
    gates(0, 0)
    gates(0, 1)
    send_carry(0)

    @at_mid
    def _():
        mid_pump(2, 2, 0)
        arrived(1)
        lent_out[1] = project(1, nrm_lent)
        lend_back(1).start()
        gel_s[...] = jax.nn.gelu(project(1, nrm).astype(F32))
        mid_pump(3, 1, 0)
        mid_pump(3, 0, PARTS)

    @at_end
    def _():
        feed_end(4)
        end_pump(2, 3, 0)
        lend_back(1).wait_recv()
        feed_end(2)
        gel_s[...] = jax.nn.gelu(lent_in[1].astype(F32))

    take_carry(0)
    mix()

    def ahead(i):
        if i == 3:
            mid_do(M(3, 2), M(4, 1))

    project_out(0, ahead)
    mid_do(M(4, 0, PARTS))
    end_do(F(2))
    close_layer(0, x_ref)

    agx[1, t] = xs[1]
    mid_do(M(4, 2), lambda: own_out_if(5, False), M(5, 1))
    end_do(E(3, 2, 1), E(3, 3), F(99), E(4, 2), E(4, 3))
    ag_finish(1, xs.at[1])
    normalize(1, 1, nrm)
    arrived(3)
    ext[1, 8:] = project(2, nrm).astype(F32)
    send_halo(1)
    mid_do(M(5, 0), M(5, 2), lambda: own_out_if(5, True))
    end_do(E(5, 1))
    take_halo(1)
    gates(1, 0)
    gates(1, 1)
    send_carry(1)
    end_do(E(5, 2))
    arrived(4)
    gel_s[...] = jax.nn.gelu(project(3, nrm).astype(F32))
    take_carry(1)
    mix()

    def ahead_last(i):
        if i == 1:
            end_do(E(5, 3))

    project_out(1, ahead_last)
    close_layer(1, xs.at[1])

    fresh = xs[layers].astype(F32)
    square = jnp.sum(fresh * fresh, axis=1, keepdims=True)
    sq_out[...] = jnp.broadcast_to(square, (rows, 128)).T[0:8]

    def sq_copy(d):
        return pltpu.make_async_remote_copy(
            src_ref=sq_out,
            dst_ref=sq_in.at[d],
            send_sem=sem_q_send.at[d],
            recv_sem=sem_q_recv.at[d],
            device_id={"tp": lax.rem(t + d, n_tp)},
            device_id_type=MESH,
        )

    for d in range(1, n_tp):
        sq_copy(d).start()
    total = sq_out[0:1]
    for d in range(1, n_tp):
        sq_copy(d).wait_recv()
        total = total + sq_in[d, 0:1]
    inv = lax.rsqrt(total / full + EPSILON)
    inv = jnp.broadcast_to(inv, (128, rows)).T[:, 0:1]
    out_ref[...] = (xs[layers].astype(F32) * inv * final_ref[...]).astype(BF16)

    assert not end_line and not mid_in_line
    close_weights()

    @at_end
    def _():
        for h in range(BANDS):
            lend_rows(h).wait_send()

    @at_mid
    def _():
        ag_close(0, x_ref)
        ag_close(layers, agx.at[layers, t])
        for i in range(len(LENT)):
            lend_back(i).wait_send()

    for layer in range(layers):
        if layer:
            ag_close(layer, xs.at[layer])

        @pl.when((s >= first_sender(layer)) & (s < n_sp - 1))
        def _():
            halo_copy(layer).wait_send()

        for d in range(1, n_sp):

            @pl.when(s + d < n_sp)
            def _():
                carry_copy(layer, d).wait_send()

        for h in range(BANDS):
            for q in range(chips):
                near_copy(layer, q, h).wait_send()
            for q in range(1, chips):
                far_copy(layer, q, h).wait_send()
    for d in range(1, n_tp):
        sq_copy(d).wait_send()


def in_one_kernel(
    sizes_of,
    starting_stream,
    multiplier_matrix,
    memory_path_matrix,
    filter_coefficients,
    memory_valve_matrix,
    entry_valve_matrix,
    forgetting_parameters,
    timestep_forgetting_multiplier,
    spike_extra,
    exit_projector_matrix,
    prelude_rms_gains,
    finishing_rms_gains,
):
    n_grp, n_sp, n_tp = sizes_of
    rows, feats = starting_stream.shape
    layers, depth, chans = memory_path_matrix.shape
    pieces = rows // 128 if rows % 128 == 0 else 1
    sizes = (layers, n_sp, n_tp, n_grp, rows, chans, feats, depth, pieces)
    chips = n_tp // 2
    half_in = (layers, 2, depth // 2, chans)
    half_out = (layers, 2, chans // 2, depth)
    rate = -SQUASH_POWER * jax.nn.softplus(-forgetting_parameters)
    vmem = pl.BlockSpec(memory_space=pltpu.VMEM)
    hbm = pl.BlockSpec(memory_space=pl.ANY)
    count = 3 * layers
    dma = pltpu.SemaphoreType.DMA
    return pl.pallas_call(
        functools.partial(fused, sizes),
        out_shape=jax.ShapeDtypeStruct((rows, feats), BF16),
        in_specs=[vmem, hbm, hbm, hbm] + [vmem] * 8,
        out_specs=vmem,
        scratch_shapes=[
            pltpu.VMEM((2 * layers * n_sp * 2, depth // 2, chans), BF16),
            pltpu.VMEM((layers * n_sp * 2, chans // 2, depth), BF16),
            pltpu.VMEM((layers + 1, n_tp, rows, feats), BF16),
            pltpu.VMEM((layers + 1, rows, feats), BF16),
            pltpu.VMEM((rows, n_tp * feats), BF16),
            pltpu.VMEM((rows, n_tp * feats), BF16),
            pltpu.VMEM((layers, 8 + rows, chans), F32),
            pltpu.VMEM((layers, 8, chans), F32),
            pltpu.VMEM((rows, chans), F32),
            pltpu.VMEM((rows, chans), F32),
            pltpu.VMEM((rows, chans), F32),
            pltpu.VMEM((rows, chans), BF16),
            pltpu.VMEM((len(LENT), rows, chans), BF16),
            pltpu.VMEM((len(LENT), rows, chans), BF16),
            pltpu.VMEM((layers, n_tp, rows, feats), BF16),
            pltpu.VMEM((layers, chips, rows, feats), BF16),
            pltpu.VMEM((layers, chips, rows, feats), BF16),
            pltpu.VMEM((layers, chips, rows, feats), BF16),
            pltpu.VMEM((layers, 2, chans), F32),
            pltpu.VMEM((layers, n_sp, 2, chans), F32),
            pltpu.VMEM((1, chans), F32),
            pltpu.VMEM((rows, 1), F32),
            pltpu.VMEM((8, rows), F32),
            pltpu.VMEM((n_tp, 8, rows), F32),
            dma((count,)),
            dma((count, n_sp, 2, PARTS)),
            dma((3,)),
            dma((BANDS + 2 * len(LENT),)),
            dma((layers + 1, 2 * chips, BANDS)),
            dma((layers + 1, n_tp, BANDS)),
            dma((layers, 2 * chips, BANDS)),
            dma((layers, 2 * chips, BANDS)),
            dma((layers, 2)),
            dma((layers, n_sp)),
            dma((layers, n_sp)),
            dma((n_tp,)),
            dma((n_tp,)),
        ],
        compiler_params=pltpu.CompilerParams(
            collective_id=0, has_side_effects=True, vmem_limit_bytes=60 * 2**20
        ),
    )(
        starting_stream,
        multiplier_matrix.reshape(half_in),
        memory_path_matrix.reshape(half_in),
        exit_projector_matrix.reshape(half_out),
        filter_coefficients,
        memory_valve_matrix,
        entry_valve_matrix,
        rate,
        timestep_forgetting_multiplier.reshape(1, rows),
        spike_extra,
        prelude_rms_gains,
        finishing_rms_gains.reshape(1, feats),
    )


def on_each(sizes_of, *arrays):
    stream, memory = arrays[0], arrays[2]
    n_grp, n_sp, n_tp = sizes_of
    rows, feats = stream.shape
    depth, chans = memory.shape[1:]
    fits = (
        n_grp == 2
        and n_sp == 4
        and memory.shape[0] == 2
        and n_tp % 2 == 0
        and rows % 128 == 0
        and depth % 128 == 0
        and feats % 128 == 0
        and chans % BLOCK_W == 0
        and depth == feats
        and n_sp == n_tp
    )
    if fits:
        return in_one_kernel(sizes_of, *arrays)
    return on_device(*arrays)


def solution(mesh):
    sizes_of = tuple(mesh.shape[axis] for axis in ("grp", "sp", "tp"))
    body = functools.partial(on_each, sizes_of)
    return jax.shard_map(
        body,
        mesh=mesh,
        in_specs=(
            P(("grp", "sp"), "tp"),
            P(None, "sp", "tp"),
            P(None, "sp", "tp"),
            P(None, None, "tp"),
            P(None, "tp", None, None),
            P(None, "tp", None, None),
            P(None, "tp"),
            P(("grp", "sp")),
            P(("grp", "sp"), "tp"),
            P(None, "tp", "sp"),
            P(),
            P("tp"),
        ),
        out_specs=P(("grp", "sp"), "tp"),
        check_vma=False,
    )
```

```python
import functools

import jax
import jax.numpy as jnp
from jax import lax
from jax.experimental import pallas as pl
from jax.experimental.pallas import tpu as pltpu
from jax.sharding import PartitionSpec as P

BLOCK_W = 256


EPSILON = 1e-06
SQUASH_POWER = 8.0


def from_behind(value, axis, steps):
    count = lax.axis_size(axis)
    first, last = (max(0, -steps), min(count, count - steps))
    return lax.ppermute(value, axis, [(source, source + steps) for source in range(first, last)])


def entering(part, axis, combine, identity):
    place = lax.axis_index(axis)
    gathered = jax.tree.map(lambda a: lax.all_gather(a, axis), part)
    state = jax.tree.map(lambda a, e: jnp.zeros_like(a) + jnp.asarray(e, a.dtype), part, identity)

    def one(lap, state):
        return combine(
            state, jax.tree.map(lambda a: lax.dynamic_index_in_dim(a, lap, 0, False), gathered)
        )

    return lax.fori_loop(0, place, one, state)


def combine_pairs(earlier, later):
    return (earlier[0] * later[0], later[0] * earlier[1] + later[1])


def gather_rows(own_cols):
    return lax.all_gather(own_cols, "tp", axis=1, tiled=True)


def on_device(
    starting_stream,
    multiplier_matrix,
    memory_path_matrix,
    filter_coefficients,
    memory_valve_matrix,
    entry_valve_matrix,
    forgetting_parameters,
    timestep_forgetting_multiplier,
    spike_extra,
    exit_projector_matrix,
    prelude_rms_gains,
    finishing_rms_gains,
):
    tok_rows = starting_stream.shape[0]
    channels = memory_path_matrix.shape[2]
    own_cols = starting_stream
    full_rows = gather_rows(starting_stream)
    for tier_number in range(memory_path_matrix.shape[0]):
        floats = full_rows.astype(jnp.float32)
        mean_square = jnp.mean(floats * floats, axis=1, keepdims=True)
        normed = (
            floats * lax.rsqrt(mean_square + EPSILON) * prelude_rms_gains[tier_number][None, :]
        ).astype(jnp.bfloat16)
        branch_acc = jnp.dot(
            normed,
            lax.all_gather(multiplier_matrix[tier_number], "sp", axis=0, tiled=True),
            preferred_element_type=jnp.float32,
        )
        recur_acc = jnp.dot(
            normed,
            lax.all_gather(memory_path_matrix[tier_number], "sp", axis=0, tiled=True),
            preferred_element_type=jnp.float32,
        )
        branch = branch_acc.astype(jnp.bfloat16)
        recurrent = recur_acc.astype(jnp.bfloat16)
        taps_now = filter_coefficients[tier_number]
        reach_back = taps_now.shape[0] - 1
        halo_rows = from_behind(recurrent[tok_rows - reach_back :], "sp", 1)
        extended = jnp.concatenate([halo_rows, recurrent], axis=0)
        conv_sum = jnp.zeros((tok_rows, channels), jnp.float32)
        for offset in range(taps_now.shape[0]):
            conv_sum = conv_sum + extended[offset : offset + tok_rows].astype(
                jnp.float32
            ) * taps_now[offset].astype(jnp.float32)
        convolved = conv_sum.astype(jnp.bfloat16)
        blocks = convolved.reshape(tok_rows, channels // BLOCK_W, BLOCK_W)
        reset_gate = jax.nn.sigmoid(
            jnp.einsum(
                "tnc,ncd->tnd",
                blocks,
                memory_valve_matrix[tier_number],
                preferred_element_type=jnp.float32,
            ).reshape(tok_rows, channels)
        )
        inject = jax.nn.sigmoid(
            jnp.einsum(
                "tnc,ncd->tnd",
                blocks,
                entry_valve_matrix[tier_number],
                preferred_element_type=jnp.float32,
            ).reshape(tok_rows, channels)
        )
        logarithmic_persistence = (
            -SQUASH_POWER
            * reset_gate
            * jax.nn.softplus(-forgetting_parameters[tier_number])[None, :]
            * timestep_forgetting_multiplier[:, None]
            + spike_extra
        )
        keep_rate = jnp.exp(logarithmic_persistence)
        driven = (
            inject
            * convolved.astype(jnp.float32)
            * jnp.sqrt(-jnp.expm1(2.0 * logarithmic_persistence))
        )
        keep_cum, state_local = lax.associative_scan(combine_pairs, (keep_rate, driven), axis=0)
        identity = (jnp.ones((channels,), jnp.float32), jnp.zeros((channels,), jnp.float32))
        carried = entering((keep_cum[-1], state_local[-1]), "sp", combine_pairs, identity)
        state_seq = state_local + keep_cum * carried[1][None, :]
        mixed_in = (jax.nn.gelu(branch.astype(jnp.float32)) * state_seq).astype(jnp.bfloat16)
        partial_value = jnp.dot(
            mixed_in,
            lax.all_gather(exit_projector_matrix[tier_number], "sp", axis=1, tiled=True),
            preferred_element_type=jnp.float32,
        )
        mixed_sum = lax.psum_scatter(
            partial_value.astype(jnp.bfloat16), "tp", scatter_dimension=1, tiled=True
        ).astype(jnp.float32)
        own_cols = (own_cols.astype(jnp.float32) + mixed_sum).astype(jnp.bfloat16)
        if tier_number + 1 < memory_path_matrix.shape[0]:
            full_rows = gather_rows(own_cols)
    floats = own_cols.astype(jnp.float32)
    full_width = floats.shape[1] * lax.axis_size("tp")
    square_sum = lax.psum(jnp.sum(floats * floats, axis=1), "tp")
    inv_rms = lax.rsqrt(square_sum / full_width + EPSILON)
    return (floats * inv_rms[:, None] * finishing_rms_gains[None, :]).astype(jnp.bfloat16)


MESH = pl.DeviceIdType.MESH
F32, BF16 = jnp.float32, jnp.bfloat16

PARTS = 4
BANDS = 2
LENT = (0, 1)
WHOLE = (1, 2, 3, 4, 5)


def one_minus_exp(u):
    series = -u * (
        1 + u / 2 * (1 + u / 3 * (1 + u / 4 * (1 + u / 5 * (1 + u / 6 * (1 + u / 7)))))
    )
    return jnp.where(u > -0.35, series, 1.0 - jnp.exp(u))


def soft_plus(u):
    e = jnp.exp(-jnp.abs(u))
    series = jnp.zeros_like(e)
    for k in range(10, 0, -1):
        series = e * (1.0 / k - series)
    return jnp.maximum(u, 0.0) + jnp.where(e < 0.1, series, jnp.log(1.0 + e))


def shifted(value, steps, fill):
    rows = value.shape[0]
    if steps % 8 == 0:
        top = jnp.full((steps, value.shape[1]), fill, value.dtype)
        return jnp.concatenate([top, value[: rows - steps]], axis=0)
    at = lax.broadcasted_iota(jnp.int32, value.shape, 0)
    return jnp.where(at < steps, fill, pltpu.roll(value, steps, 0))


def fused(
    sizes,
    x_hbm,
    branch_w,
    memory_w,
    exit_w,
    taps_hbm,
    reset_hbm,
    inject_hbm,
    forget_hbm,
    mult_hbm,
    spike_hbm,
    gains_hbm,
    final_hbm,
    out_ref,
    x_ref,
    taps_ref,
    reset_w,
    inject_w,
    rate_ref,
    mult_ref,
    spike_ref,
    gains_ref,
    final_ref,
    win,
    wout,
    agx,
    xs,
    nrm,
    nrm_lent,
    ext,
    halo,
    keep_s,
    state_s,
    gel_s,
    mix_s,
    lent_out,
    lent_in,
    part,
    from_sib,
    pair,
    from_far,
    cry_out,
    cry_in,
    hacc,
    mult_s,
    sq_out,
    sq_in,
    sem_load,
    sem_own,
    sem_piece,
    sem_rest,
    sem_w_send,
    sem_lend,
    sem_ag_send,
    sem_ag_recv,
    sem_rs_send,
    sem_rs_recv,
    sem_h,
    sem_c_send,
    sem_c_recv,
    sem_q_send,
    sem_q_recv,
):
    layers, n_sp, n_tp, n_grp, rows, chans, feats, depth, pieces = sizes
    chips = n_tp // 2
    count = 3 * layers
    g, s, t = lax.axis_index("grp"), lax.axis_index("sp"), lax.axis_index("tp")
    core = lax.rem(t, 2)
    chip = t // 2
    sib = chip * 2 + 1 - core
    full = n_tp * feats
    inw = 1 - 2 * (s // (n_sp // 2))
    is_end = (s == 0) | (s == n_sp - 1)
    is_mid = (s > 0) & (s < n_sp - 1)

    def at_end(body):
        pl.when(is_end)(body)

    def at_mid(body):
        pl.when(is_mid)(body)

    def own_block(m):
        return (memory_w, branch_w, exit_w)[m % 3].at[m // 3]

    def slot(m, j):
        kind = 2 * (m // 3) + m % 3 if m % 3 < 2 else m // 3
        return (win if m % 3 < 2 else wout), (kind * n_sp + j) * 2

    def keep_own(m):
        ref, at = slot(m, s)
        return pltpu.make_async_copy(own_block(m), ref.at[pl.ds(at, 2)], sem_own.at[m])

    loads = [
        pltpu.make_async_copy(src, dst, sem_load.at[i])
        for i, (src, dst) in enumerate(
            (
                (x_hbm, x_ref),
                (gains_hbm, gains_ref),
                (mult_hbm, mult_ref),
                (forget_hbm, rate_ref),
                (taps_hbm, taps_ref),
                (reset_hbm, reset_w),
                (inject_hbm, inject_w),
                (spike_hbm, spike_ref),
                (final_hbm, final_ref),
            )
        )
    ]
    barrier = pltpu.get_barrier_semaphore()
    for d in range(1, n_tp):
        pl.semaphore_signal(
            barrier, inc=1, device_id={"tp": lax.rem(t + d, n_tp)}, device_id_type=MESH
        )
    for d in range(1, n_sp):
        pl.semaphore_signal(
            barrier, inc=1, device_id={"sp": lax.rem(s + d, n_sp)}, device_id_type=MESH
        )
    pl.semaphore_signal(barrier, inc=1, device_id={"grp": 1 - g}, device_id_type=MESH)
    for load in loads:
        load.start()
    for m in range(len(LENT), 3 * layers):
        keep_own(m).start()
    pl.semaphore_wait(barrier, n_tp - 1 + n_sp - 1 + 1)

    IN, OUT, ACROSS = 0, 1, 2

    def target(way):
        if way == ACROSS:
            return {"grp": 1 - g}
        return {"sp": s + inw} if way == IN else {"sp": s - inw}

    def cut(ref, q):
        size = ref.shape[0] // PARTS
        return ref.at[pl.ds(q * size, size)]

    def held(m, j, half, q):
        ref, at = slot(m, j)
        return cut(ref.at[at + half], q)

    def arrival(m, j, place, mine, q):
        away = lax.rem(j - place + 2 * n_sp - 1, n_sp)
        return sem_piece.at[m, away, q] if mine else sem_rest.at[m, away]

    def sent(src, m, j, half, q, way, mine):
        place = s + (inw, -inw, 0)[way]
        return pltpu.make_async_remote_copy(
            src_ref=src,
            dst_ref=held(m, j, half, q),
            send_sem=sem_w_send.at[way],
            recv_sem=arrival(m, j, place, mine, q),
            device_id=target(way),
            device_id_type=MESH,
        )

    def relay(m, j, q, ways):
        src = held(m, j, g, q)
        for way in ways:
            sent(src, m, j, g, q, way, way != ACROSS).start()

    def landed(m, j, q):
        piece = held(m, j, g, q)
        sent(piece, m, j, g, q, ACROSS, True).wait_recv()

    def own(m, way, half, q):
        src = cut(own_block(m).at[half], q)
        sent(src, m, s, half, q, way, half is g).start()

    def own_both(m, way):
        for q in range(PARTS):
            own(m, way, g, q)

    halves = [(1, g)]
    for m in range(2, count):
        halves += [(m, g), (m - 1, 1 - g)]
    halves.append((count - 1, 1 - g))
    end_line = [(m, half, q) for m, half in halves for q in range(PARTS)]
    mid_in_line = [(m, q) for m in (2, 1, *range(3, count)) for q in range(PARTS)]
    def feed_end(steps):
        steps *= PARTS // 2
        for m, half, q in end_line[:steps]:
            own(m, IN, half, q)
        del end_line[:steps]

    def feed_in(steps):
        for m, q in mid_in_line[:steps]:
            own(m, IN, g, q)
        del mid_in_line[:steps]

    def end_pump(m, i, feed, pieces=range(PARTS)):
        j = s + inw * i
        for q in pieces:
            landed(m, j, q)
            relay(m, j, q, (ACROSS,))
            if q % (PARTS // 2) == PARTS // 2 - 1:
                feed_end(feed)

    def mid_block(k):
        return s + inw * (k if k else -1)

    def mid_ways(m, k):
        if k == 0:
            return (IN,) if m in WHOLE else (IN, ACROSS)
        return (ACROSS,) if m in LENT else (OUT, ACROSS)

    def mid_pump(m, k, feed, pieces=range(PARTS)):
        for q in pieces:
            landed(m, mid_block(k), q)
            relay(m, mid_block(k), q, mid_ways(m, k))
        feed_in(feed)

    def end_do(*acts):
        def body():
            for act in acts:
                act()

        at_end(body)

    def mid_do(*acts):
        def body():
            for act in acts:
                act()

        at_mid(body)

    def E(m, i, feed=0):
        return lambda: end_pump(m, i, feed)

    def M(m, k, feed=0):
        return lambda: mid_pump(m, k, feed)

    def F(steps):
        return lambda: feed_end(steps)

    def ready(m, j):
        ref, at = slot(m, j)
        rest = ref.at[at + 1 - g]
        pltpu.make_async_remote_copy(
            src_ref=rest,
            dst_ref=rest,
            send_sem=sem_w_send.at[ACROSS],
            recv_sem=arrival(m, j, s, False, 0),
            device_id=target(ACROSS),
            device_id_type=MESH,
        ).wait_recv()

    def arrived(m):
        keep_own(m).wait()
        for d in range(1, n_sp):
            ready(m, lax.rem(s + d, n_sp))

    def wait_sends(way, halves):
        view = win.at[pl.ds(0, halves)]
        pltpu.make_async_remote_copy(
            src_ref=view,
            dst_ref=view,
            send_sem=sem_w_send.at[way],
            recv_sem=sem_rest.at[0, 0],
            device_id=target(ACROSS),
            device_id_type=MESH,
        ).wait_send()

    def close_weights():
        lent, whole = len(LENT), len(WHOLE)

        @at_end
        def _():
            wait_sends(IN, count + whole)
            wait_sends(ACROSS, (count - lent) * (n_sp - 1))

        @at_mid
        def _():
            wait_sends(IN, 2 * count)
            wait_sends(OUT, (count - lent) * (n_sp - 1))
            wait_sends(ACROSS, count * (n_sp - 1) - whole)

    def band(ref, h):
        return ref.at[pl.ds(h * (rows // BANDS), rows // BANDS)]

    def ag_copy(src, layer, owner, h, where):
        return pltpu.make_async_remote_copy(
            src_ref=band(src, h),
            dst_ref=band(agx.at[layer, owner], h),
            send_sem=sem_ag_send.at[layer],
            recv_sem=sem_ag_recv.at[layer, owner, h],
            device_id={"tp": where},
            device_id_type=MESH,
        )

    def ag_start(layer, src, h):
        for d in range(1, chips):
            ag_copy(src, layer, t, h, lax.rem(t + 2 * d, n_tp)).start()
        ag_copy(src, layer, t, h, sib).start()

    def ag_forward(layer):
        for h in range(BANDS):
            for d in range(1, chips):
                owner = lax.rem(t + 2 * d, n_tp)
                block = agx.at[layer, owner]
                ag_copy(block, layer, owner, h, sib).wait_recv()
                ag_copy(block, layer, owner, h, sib).start()

    def ag_finish(layer, src):
        for h in range(BANDS):
            ag_copy(src, layer, sib, h, sib).wait_recv()
            for d in range(1, chips):
                owner = lax.rem(sib + 2 * d, n_tp)
                ag_copy(agx.at[layer, owner], layer, owner, h, sib).wait_recv()

    def wait_blocks(view, sem):
        pltpu.make_async_remote_copy(
            src_ref=view,
            dst_ref=view,
            send_sem=sem,
            recv_sem=sem_rest.at[0, 0],
            device_id=target(ACROSS),
            device_id_type=MESH,
        ).wait_send()

    def ag_close(layer):
        wait_blocks(agx.at[layer, pl.ds(0, 2 * chips - 1)], sem_ag_send.at[layer])

    def lend_rows(h):
        return pltpu.make_async_remote_copy(
            src_ref=band(x_ref, h),
            dst_ref=band(agx.at[layers, t], h),
            send_sem=sem_lend.at[h],
            recv_sem=sem_ag_recv.at[layers, t, h],
            device_id=target(IN),
            device_id_type=MESH,
        )

    def lend_back(i):
        return pltpu.make_async_remote_copy(
            src_ref=lent_out.at[i],
            dst_ref=lent_in.at[i],
            send_sem=sem_lend.at[BANDS + i],
            recv_sem=sem_lend.at[BANDS + len(LENT) + i],
            device_id=target(OUT),
            device_id_type=MESH,
        )

    step = rows // pieces

    def normalize(layer, gain_row, nrm):
        def one(i, carry):
            at = pl.ds(pl.multiple_of(i * step, step), step)
            total = jnp.zeros((step, 1), F32)
            for p in range(n_tp):
                f = agx[layer, p, at].astype(F32)
                total = total + jnp.sum(f * f, axis=1, keepdims=True)
            inv = lax.rsqrt(total / full + EPSILON)
            for p in range(n_tp):
                cols = slice(p * feats, (p + 1) * feats)
                f = agx[layer, p, at].astype(F32)
                gain = gains_ref[gain_row : gain_row + 1, cols]
                nrm[at, cols] = (f * inv * gain).astype(BF16)
            return carry

        lax.fori_loop(0, pieces, one, 0)

    def project(idx, nrm):
        total = None
        for j in range(n_sp):
            at = (idx * n_sp + j) * 2
            term = jnp.dot(
                nrm[:, j * depth : (j + 1) * depth],
                win[at : at + 2].reshape(depth, chans),
                preferred_element_type=F32,
            )
            total = term if total is None else total + term
        return total.astype(BF16)

    def halo_copy(layer):
        return pltpu.make_async_remote_copy(
            src_ref=ext.at[layer, pl.ds(rows, 8)],
            dst_ref=halo.at[layer],
            send_sem=sem_h.at[layer, 0],
            recv_sem=sem_h.at[layer, 1],
            device_id={"sp": s + 1},
            device_id_type=MESH,
        )

    def carry_copy(layer, d):
        return pltpu.make_async_remote_copy(
            src_ref=cry_out.at[layer],
            dst_ref=cry_in.at[layer, s],
            send_sem=sem_c_send.at[layer, d],
            recv_sem=sem_c_recv.at[layer, s],
            device_id={"sp": s + d},
            device_id_type=MESH,
        )

    def carry_wait(layer, j):
        pltpu.make_async_remote_copy(
            src_ref=cry_out.at[layer],
            dst_ref=cry_in.at[layer, j],
            send_sem=sem_c_send.at[layer, 0],
            recv_sem=sem_c_recv.at[layer, j],
            device_id={"sp": s},
            device_id_type=MESH,
        ).wait_recv()

    def rs_copy(src, dst, layer, k, h, where):
        return pltpu.make_async_remote_copy(
            src_ref=src,
            dst_ref=dst,
            send_sem=sem_rs_send.at[layer],
            recv_sem=sem_rs_recv.at[layer, k, h],
            device_id={"tp": where},
            device_id_type=MESH,
        )

    def near_copy(layer, q, h):
        to = lax.rem(sib + 2 * q, n_tp)
        src, dst = band(part.at[layer, to], h), band(from_sib.at[layer, q], h)
        return rs_copy(src, dst, layer, q, h, sib)

    def far_copy(layer, q, h):
        where = lax.rem(t + 2 * q, n_tp)
        src, dst = band(pair.at[layer, q], h), band(from_far.at[layer, q], h)
        return rs_copy(src, dst, layer, chips + q - 1, h, where)

    def first_sender(layer):
        return 1 if layer == 0 else 0

    def send_halo(layer):
        @pl.when((s >= first_sender(layer)) & (s < n_sp - 1))
        def _():
            halo_copy(layer).start()

    def take_halo(layer):
        @pl.when(s == 0)
        def _():
            halo[layer] = jnp.zeros((8, chans), F32)

        if layer == 0:

            @pl.when(s == 1)
            def _():
                halo[layer] = lent_out[0].astype(F32)[rows - 8 :]

        @pl.when(s > first_sender(layer))
        def _():
            halo_copy(layer).wait_recv()

        ext[layer, :8] = halo[layer]

    def gates(layer, b):
        n_taps = taps_ref.shape[1]
        base = 8 - (n_taps - 1)
        cols = slice(b * BLOCK_W, (b + 1) * BLOCK_W)
        conv = jnp.zeros((rows, BLOCK_W), F32)
        for k in range(n_taps):
            tap = taps_ref[layer, k : k + 1, cols].astype(F32)
            conv = conv + ext[layer, base + k : base + k + rows, cols] * tap
        conv = conv.astype(BF16)
        reset = jax.nn.sigmoid(
            jnp.dot(conv, reset_w[layer, b], preferred_element_type=F32)
        )
        inject = jax.nn.sigmoid(
            jnp.dot(conv, inject_w[layer, b], preferred_element_type=F32)
        )
        log_keep = (
            reset * rate_ref[layer : layer + 1, cols] * mult_s[...] + spike_ref[:, cols]
        )
        keep = jnp.exp(log_keep)
        state = inject * conv.astype(F32) * jnp.sqrt(one_minus_exp(2.0 * log_keep))
        lag = 1
        while lag < rows:
            state = keep * shifted(state, lag, 0.0) + state
            keep = keep * shifted(keep, lag, 1.0)
            lag *= 2
        keep_s[:, cols] = keep
        state_s[:, cols] = state
        cry_out[layer, 0:1, cols] = keep[rows - 1 :]
        cry_out[layer, 1:2, cols] = state[rows - 1 :]

    def send_carry(layer):
        for d in range(1, n_sp):

            @pl.when(s + d < n_sp)
            def _():
                carry_copy(layer, d).start()

    def take_carry(layer):
        hacc[...] = jnp.zeros((1, chans), F32)
        for j in range(n_sp - 1):

            @pl.when(j < s)
            def _():
                carry_wait(layer, j)
                hacc[...] = cry_in[layer, j, 0:1] * hacc[...] + cry_in[layer, j, 1:2]

    def mix():
        mix_s[...] = (
            gel_s[...] * (state_s[...] + keep_s[...] * hacc[...])
        ).astype(BF16)

    def chips_on(j):
        return lax.rem(j // 2 - chip + chips, chips)

    def product(layer, j):
        at = (layer * n_sp + j) * 2
        part[layer, j] = jnp.dot(
            mix_s[...],
            wout[pl.ds(at, 2)].reshape(chans, depth),
            preferred_element_type=F32,
        ).astype(BF16)

        @pl.when(lax.rem(j, 2) != core)
        def _():
            for h in range(BANDS):
                near_copy(layer, chips_on(j), h).start()

    def pass_on(layer, j):
        q = chips_on(j)

        @pl.when((lax.rem(j, 2) == core) & (q != 0))
        def _():
            for h in range(BANDS):
                at = pl.ds(h * (rows // BANDS), rows // BANDS)
                near_copy(layer, q, h).wait_recv()
                pair[layer, q, at] = (
                    part[layer, j, at].astype(F32) + from_sib[layer, q, at].astype(F32)
                ).astype(BF16)
                far_copy(layer, q, h).start()

    def crossing_order(i):
        there = 2 * (1 - chip) if i < 2 else 2 * chip
        return there + (core if i % 2 else 1 - core)

    def project_out(layer, ahead):
        m = 3 * layer + 2
        e = is_end.astype(jnp.int32)
        turned = (chip == s // (n_tp // chips)).astype(jnp.int32)
        keep_own(m).wait()

        @at_mid
        def _():
            for d in range(1, n_sp):
                ready(m, lax.rem(s + d, n_sp))

        waiting = []
        for i in range(n_sp):
            step = (0, 1, 2, 3)[i] + turned * (2, -1, -1, 0)[i]
            j = s + inw * step
            ahead(i)
            pl.when(is_end & (step > 0))(functools.partial(ready, m, j))
            j = crossing_order(i) + e * (j - crossing_order(i))
            product(layer, j)
            waiting.append(j)
            if i:
                for done in waiting:
                    pass_on(layer, done)
                waiting = []

    def close_layer(layer, src, ahead):
        for h in range(BANDS):
            ahead(h)
            at = pl.ds(h * (rows // BANDS), rows // BANDS)
            near_copy(layer, 0, h).wait_recv()
            mixed = part[layer, t, at].astype(F32) + from_sib[layer, 0, at].astype(F32)
            for q in range(1, chips):
                far_copy(layer, q, h).wait_recv()
                mixed = mixed + from_far[layer, q, at].astype(F32)
            xs[layer + 1, at] = (src[at].astype(F32) + mixed).astype(BF16)
            if layer + 1 < layers:
                ag_start(layer + 1, xs.at[layer + 1], h)

    own_both(0, IN)
    loads[0].wait()

    @at_end
    def _():
        for h in range(BANDS):
            lend_rows(h).start()
        feed_end(2)

    @at_mid
    def _():
        for h in range(BANDS):
            ag_start(0, x_ref, h)
        for m in range(len(LENT), count - 1):
            own_both(m, OUT)
        for m in LENT:
            keep_own(m).start()
        agx[0, t] = x_ref[...]

    for load in loads[1:]:
        load.wait()
    rate_ref[...] = -SQUASH_POWER * soft_plus(-rate_ref[...])
    mult_s[...] = jnp.broadcast_to(mult_ref[...].reshape(1, rows), (128, rows)).T[:, 0:1]

    @at_mid
    def _():
        mid_pump(0, 0, PARTS)
        mid_pump(0, 1, 0)
        ag_forward(0)
        ag_finish(0, x_ref)
        normalize(0, 0, nrm)
        lend_rows(0).wait_recv()
        ag_start(layers, agx.at[layers, t], 0)
        mid_pump(0, 2, PARTS)
        for h in range(1, BANDS):
            lend_rows(h).wait_recv()
            ag_start(layers, agx.at[layers, t], h)
        for q in range(PARTS):
            landed(2, mid_block(1), q)
            relay(2, mid_block(1), q, (OUT,))
        own_both(count - 1, OUT)
        ag_forward(layers)
        arrived(0)
        ext[0, 8:] = project(0, nrm).astype(F32)
        send_halo(0)
        for q in range(PARTS):
            landed(1, mid_block(1), q)
            relay(1, mid_block(1), q, mid_ways(1, 1))
            landed(1, mid_block(0), q)
            relay(1, mid_block(0), q, mid_ways(1, 0))
        ag_finish(layers, agx.at[layers, t])
        normalize(layers, 0, nrm_lent)
        lent_out[0] = project(0, nrm_lent)
        lend_back(0).start()
        mid_pump(2, 0, PARTS)
        mid_pump(1, 2, 0)
        for q in range(PARTS):
            relay(2, mid_block(1), q, (ACROSS,))

    @at_end
    def _():
        end_pump(2, 1, 0)
        end_pump(3, 1, 0)
        end_pump(4, 1, 1)
        feed_end(2)
        end_pump(2, 2, 1)
        feed_end(2)
        end_pump(5, 1, 0)
        lend_back(0).wait_recv()
        ext[0, 8:] = lent_in[0].astype(F32)

    take_halo(0)
    gates(0, 0)
    gates(0, 1)
    send_carry(0)

    @at_mid
    def _():
        mid_pump(2, 2, 0, range(PARTS // 2))
        arrived(1)
        lent_out[1] = project(1, nrm_lent)
        lend_back(1).start()
        mid_pump(2, 2, 0, range(PARTS // 2, PARTS))
        gel_s[...] = jax.nn.gelu(project(1, nrm).astype(F32))
        mid_pump(3, 1, 0)
        mid_pump(3, 0, PARTS)

    @at_end
    def _():
        feed_end(4)
        end_pump(2, 3, 0, range(PARTS // 2))
        lend_back(1).wait_recv()
        feed_end(2)
        gel_s[...] = jax.nn.gelu(lent_in[1].astype(F32))

    take_carry(0)
    mix()

    last_pieces = [
        (m, i, q) for m, i in ((4, 3), (5, 2), (5, 3)) for q in range(PARTS)
    ]

    def end_last(steps):
        @at_end
        def _():
            for m, i, q in last_pieces[:steps]:
                landed(m, s + inw * i, q)
                relay(m, s + inw * i, q, (ACROSS,))

        del last_pieces[:steps]

    def nothing(_):
        return

    def between(h):
        if h == 0:
            end_do(F(2), lambda: end_pump(3, 2, 0, range(PARTS // 2, PARTS)))
            mid_do(M(3, 2))
        turned = chip == s // (n_tp // chips)
        if h == 0:
            pl.when(is_end & jnp.logical_not(turned))(E(3, 3))
        if h == BANDS - 1:
            pl.when(is_end & turned)(E(3, 3))
            mid_do(M(4, 1), M(4, 0, PARTS))

    def rest_ahead(i):
        if i == n_sp - 1:
            end_do(lambda: end_pump(2, 3, 0, range(PARTS // 2, PARTS)), F(2))
            end_do(lambda: end_pump(3, 2, 0, range(PARTS // 2)))

    project_out(0, rest_ahead)
    close_layer(0, x_ref, between)

    agx[1, t] = xs[1]
    mid_do(M(4, 2), M(5, 0))
    end_do(F(99), E(4, 2))
    end_last(1)
    ag_forward(1)
    ag_finish(1, xs.at[1])
    end_last(1)
    normalize(1, 1, nrm)
    end_last(1)
    arrived(3)
    ext[1, 8:] = project(2, nrm).astype(F32)
    send_halo(1)
    mid_do(M(5, 1))
    pl.when(s == 1)(M(5, 2))
    end_last(1)
    take_halo(1)
    gates(1, 0)
    end_last(1)
    gates(1, 1)
    send_carry(1)
    pl.when(is_mid & (s > 1))(M(5, 2))
    end_last(1)
    arrived(4)
    end_last(1)
    gel_s[...] = jax.nn.gelu(project(3, nrm).astype(F32))
    end_last(2)
    take_carry(1)
    mix()

    def last_ahead(i):
        if i < n_sp - 1:
            end_last(1)

    project_out(1, last_ahead)
    close_layer(1, xs.at[1], nothing)

    fresh = xs[layers].astype(F32)
    square = jnp.sum(fresh * fresh, axis=1, keepdims=True)
    sq_out[...] = jnp.broadcast_to(square, (rows, 128)).T[0:8]

    def sq_copy(d):
        return pltpu.make_async_remote_copy(
            src_ref=sq_out,
            dst_ref=sq_in.at[d],
            send_sem=sem_q_send.at[d],
            recv_sem=sem_q_recv.at[d],
            device_id={"tp": lax.rem(t + d, n_tp)},
            device_id_type=MESH,
        )

    for d in range(1, n_tp):
        sq_copy(d).start()
    total = sq_out[0:1]
    for d in range(1, n_tp):
        sq_copy(d).wait_recv()
        total = total + sq_in[d, 0:1]
    inv = lax.rsqrt(total / full + EPSILON)
    inv = jnp.broadcast_to(inv, (128, rows)).T[:, 0:1]
    out_ref[...] = (xs[layers].astype(F32) * inv * final_ref[...]).astype(BF16)

    assert not end_line and not mid_in_line and not last_pieces
    close_weights()

    @at_end
    def _():
        for h in range(BANDS):
            lend_rows(h).wait_send()

    @at_mid
    def _():
        ag_close(0)
        ag_close(layers)
        for i in range(len(LENT)):
            lend_back(i).wait_send()

    for layer in range(layers):
        if layer:
            ag_close(layer)

        @pl.when((s >= first_sender(layer)) & (s < n_sp - 1))
        def _():
            halo_copy(layer).wait_send()

        for d in range(1, n_sp):

            @pl.when(s + d < n_sp)
            def _():
                carry_copy(layer, d).wait_send()

        wait_blocks(part.at[layer, pl.ds(0, 2 * chips - 1)], sem_rs_send.at[layer])
    for d in range(1, n_tp):
        sq_copy(d).wait_send()


def in_one_kernel(
    sizes_of,
    starting_stream,
    multiplier_matrix,
    memory_path_matrix,
    filter_coefficients,
    memory_valve_matrix,
    entry_valve_matrix,
    forgetting_parameters,
    timestep_forgetting_multiplier,
    spike_extra,
    exit_projector_matrix,
    prelude_rms_gains,
    finishing_rms_gains,
):
    n_grp, n_sp, n_tp = sizes_of
    rows, feats = starting_stream.shape
    layers, depth, chans = memory_path_matrix.shape
    pieces = rows // 128 if rows % 128 == 0 else 1
    sizes = (layers, n_sp, n_tp, n_grp, rows, chans, feats, depth, pieces)
    chips = n_tp // 2
    half_in = (layers, 2, depth // 2, chans)
    half_out = (layers, 2, chans // 2, depth)
    vmem = pl.BlockSpec(memory_space=pltpu.VMEM)
    hbm = pl.BlockSpec(memory_space=pl.ANY)
    count = 3 * layers
    dma = pltpu.SemaphoreType.DMA
    return pl.pallas_call(
        functools.partial(fused, sizes),
        out_shape=jax.ShapeDtypeStruct((rows, feats), BF16),
        in_specs=[hbm] * 12,
        out_specs=vmem,
        scratch_shapes=[
            pltpu.VMEM((rows, feats), BF16),
            pltpu.VMEM(filter_coefficients.shape, BF16),
            pltpu.VMEM(memory_valve_matrix.shape, BF16),
            pltpu.VMEM(entry_valve_matrix.shape, BF16),
            pltpu.VMEM((layers, chans), F32),
            pltpu.VMEM((rows,), F32),
            pltpu.VMEM((rows, chans), F32),
            pltpu.VMEM((layers, n_tp * feats), F32),
            pltpu.VMEM((1, feats), F32),
            pltpu.VMEM((2 * layers * n_sp * 2, depth // 2, chans), BF16),
            pltpu.VMEM((layers * n_sp * 2, chans // 2, depth), BF16),
            pltpu.VMEM((layers + 1, n_tp, rows, feats), BF16),
            pltpu.VMEM((layers + 1, rows, feats), BF16),
            pltpu.VMEM((rows, n_tp * feats), BF16),
            pltpu.VMEM((rows, n_tp * feats), BF16),
            pltpu.VMEM((layers, 8 + rows, chans), F32),
            pltpu.VMEM((layers, 8, chans), F32),
            pltpu.VMEM((rows, chans), F32),
            pltpu.VMEM((rows, chans), F32),
            pltpu.VMEM((rows, chans), F32),
            pltpu.VMEM((rows, chans), BF16),
            pltpu.VMEM((len(LENT), rows, chans), BF16),
            pltpu.VMEM((len(LENT), rows, chans), BF16),
            pltpu.VMEM((layers, n_tp, rows, feats), BF16),
            pltpu.VMEM((layers, chips, rows, feats), BF16),
            pltpu.VMEM((layers, chips, rows, feats), BF16),
            pltpu.VMEM((layers, chips, rows, feats), BF16),
            pltpu.VMEM((layers, 2, chans), F32),
            pltpu.VMEM((layers, n_sp, 2, chans), F32),
            pltpu.VMEM((1, chans), F32),
            pltpu.VMEM((rows, 1), F32),
            pltpu.VMEM((8, rows), F32),
            pltpu.VMEM((n_tp, 8, rows), F32),
            dma((9,)),
            dma((count,)),
            dma((count, n_sp - 1, PARTS)),
            dma((count, n_sp - 1)),
            dma((3,)),
            dma((BANDS + 2 * len(LENT),)),
            dma((layers + 1,)),
            dma((layers + 1, n_tp, BANDS)),
            dma((layers,)),
            dma((layers, 2 * chips - 1, BANDS)),
            dma((layers, 2)),
            dma((layers, n_sp)),
            dma((layers, n_sp)),
            dma((n_tp,)),
            dma((n_tp,)),
        ],
        compiler_params=pltpu.CompilerParams(
            collective_id=0, has_side_effects=True, vmem_limit_bytes=60 * 2**20
        ),
    )(
        starting_stream,
        multiplier_matrix.reshape(half_in),
        memory_path_matrix.reshape(half_in),
        exit_projector_matrix.reshape(half_out),
        filter_coefficients,
        memory_valve_matrix,
        entry_valve_matrix,
        forgetting_parameters,
        timestep_forgetting_multiplier,
        spike_extra,
        prelude_rms_gains,
        finishing_rms_gains.reshape(1, feats),
    )


def on_each(sizes_of, *arrays):
    stream, memory = arrays[0], arrays[2]
    n_grp, n_sp, n_tp = sizes_of
    rows, feats = stream.shape
    depth, chans = memory.shape[1:]
    fits = (
        n_grp == 2
        and n_sp == 4
        and memory.shape[0] == 2
        and n_tp % 2 == 0
        and rows % 128 == 0
        and depth % 128 == 0
        and feats % 128 == 0
        and chans % BLOCK_W == 0
        and depth == feats
        and n_sp == n_tp
    )
    if fits:
        return in_one_kernel(sizes_of, *arrays)
    return on_device(*arrays)


def solution(mesh):
    sizes_of = tuple(mesh.shape[axis] for axis in ("grp", "sp", "tp"))
    body = functools.partial(on_each, sizes_of)
    return jax.shard_map(
        body,
        mesh=mesh,
        in_specs=(
            P(("grp", "sp"), "tp"),
            P(None, "sp", "tp"),
            P(None, "sp", "tp"),
            P(None, None, "tp"),
            P(None, "tp", None, None),
            P(None, "tp", None, None),
            P(None, "tp"),
            P(("grp", "sp")),
            P(("grp", "sp"), "tp"),
            P(None, "tp", "sp"),
            P(),
            P("tp"),
        ),
        out_specs=P(("grp", "sp"), "tp"),
        check_vma=False,
    )
```

```python
import functools

import jax
import jax.numpy as jnp
from jax import lax
from jax.experimental import pallas as pl
from jax.experimental.pallas import tpu as pltpu
from jax.sharding import PartitionSpec as P

BLOCK_W = 256


EPSILON = 1e-06
SQUASH_POWER = 8.0


def from_behind(value, axis, steps):
    count = lax.axis_size(axis)
    first, last = (max(0, -steps), min(count, count - steps))
    return lax.ppermute(value, axis, [(source, source + steps) for source in range(first, last)])


def entering(part, axis, combine, identity):
    place = lax.axis_index(axis)
    gathered = jax.tree.map(lambda a: lax.all_gather(a, axis), part)
    state = jax.tree.map(lambda a, e: jnp.zeros_like(a) + jnp.asarray(e, a.dtype), part, identity)

    def one(lap, state):
        return combine(
            state, jax.tree.map(lambda a: lax.dynamic_index_in_dim(a, lap, 0, False), gathered)
        )

    return lax.fori_loop(0, place, one, state)


def combine_pairs(earlier, later):
    return (earlier[0] * later[0], later[0] * earlier[1] + later[1])


def gather_rows(own_cols):
    return lax.all_gather(own_cols, "tp", axis=1, tiled=True)


def on_device(
    starting_stream,
    multiplier_matrix,
    memory_path_matrix,
    filter_coefficients,
    memory_valve_matrix,
    entry_valve_matrix,
    forgetting_parameters,
    timestep_forgetting_multiplier,
    spike_extra,
    exit_projector_matrix,
    prelude_rms_gains,
    finishing_rms_gains,
):
    tok_rows = starting_stream.shape[0]
    channels = memory_path_matrix.shape[2]
    own_cols = starting_stream
    full_rows = gather_rows(starting_stream)
    for tier_number in range(memory_path_matrix.shape[0]):
        floats = full_rows.astype(jnp.float32)
        mean_square = jnp.mean(floats * floats, axis=1, keepdims=True)
        normed = (
            floats * lax.rsqrt(mean_square + EPSILON) * prelude_rms_gains[tier_number][None, :]
        ).astype(jnp.bfloat16)
        branch_acc = jnp.dot(
            normed,
            lax.all_gather(multiplier_matrix[tier_number], "sp", axis=0, tiled=True),
            preferred_element_type=jnp.float32,
        )
        recur_acc = jnp.dot(
            normed,
            lax.all_gather(memory_path_matrix[tier_number], "sp", axis=0, tiled=True),
            preferred_element_type=jnp.float32,
        )
        branch = branch_acc.astype(jnp.bfloat16)
        recurrent = recur_acc.astype(jnp.bfloat16)
        taps_now = filter_coefficients[tier_number]
        reach_back = taps_now.shape[0] - 1
        halo_rows = from_behind(recurrent[tok_rows - reach_back :], "sp", 1)
        extended = jnp.concatenate([halo_rows, recurrent], axis=0)
        conv_sum = jnp.zeros((tok_rows, channels), jnp.float32)
        for offset in range(taps_now.shape[0]):
            conv_sum = conv_sum + extended[offset : offset + tok_rows].astype(
                jnp.float32
            ) * taps_now[offset].astype(jnp.float32)
        convolved = conv_sum.astype(jnp.bfloat16)
        blocks = convolved.reshape(tok_rows, channels // BLOCK_W, BLOCK_W)
        reset_gate = jax.nn.sigmoid(
            jnp.einsum(
                "tnc,ncd->tnd",
                blocks,
                memory_valve_matrix[tier_number],
                preferred_element_type=jnp.float32,
            ).reshape(tok_rows, channels)
        )
        inject = jax.nn.sigmoid(
            jnp.einsum(
                "tnc,ncd->tnd",
                blocks,
                entry_valve_matrix[tier_number],
                preferred_element_type=jnp.float32,
            ).reshape(tok_rows, channels)
        )
        logarithmic_persistence = (
            -SQUASH_POWER
            * reset_gate
            * jax.nn.softplus(-forgetting_parameters[tier_number])[None, :]
            * timestep_forgetting_multiplier[:, None]
            + spike_extra
        )
        keep_rate = jnp.exp(logarithmic_persistence)
        driven = (
            inject
            * convolved.astype(jnp.float32)
            * jnp.sqrt(-jnp.expm1(2.0 * logarithmic_persistence))
        )
        keep_cum, state_local = lax.associative_scan(combine_pairs, (keep_rate, driven), axis=0)
        identity = (jnp.ones((channels,), jnp.float32), jnp.zeros((channels,), jnp.float32))
        carried = entering((keep_cum[-1], state_local[-1]), "sp", combine_pairs, identity)
        state_seq = state_local + keep_cum * carried[1][None, :]
        mixed_in = (jax.nn.gelu(branch.astype(jnp.float32)) * state_seq).astype(jnp.bfloat16)
        partial_value = jnp.dot(
            mixed_in,
            lax.all_gather(exit_projector_matrix[tier_number], "sp", axis=1, tiled=True),
            preferred_element_type=jnp.float32,
        )
        mixed_sum = lax.psum_scatter(
            partial_value.astype(jnp.bfloat16), "tp", scatter_dimension=1, tiled=True
        ).astype(jnp.float32)
        own_cols = (own_cols.astype(jnp.float32) + mixed_sum).astype(jnp.bfloat16)
        if tier_number + 1 < memory_path_matrix.shape[0]:
            full_rows = gather_rows(own_cols)
    floats = own_cols.astype(jnp.float32)
    full_width = floats.shape[1] * lax.axis_size("tp")
    square_sum = lax.psum(jnp.sum(floats * floats, axis=1), "tp")
    inv_rms = lax.rsqrt(square_sum / full_width + EPSILON)
    return (floats * inv_rms[:, None] * finishing_rms_gains[None, :]).astype(jnp.bfloat16)


MESH = pl.DeviceIdType.MESH
F32, BF16 = jnp.float32, jnp.bfloat16

PARTS = 4
BANDS = 2
LENT = (0, 1)
WHOLE = (1, 2, 3, 4, 5)


def one_minus_exp(u):
    series = -u * (
        1 + u / 2 * (1 + u / 3 * (1 + u / 4 * (1 + u / 5 * (1 + u / 6 * (1 + u / 7)))))
    )
    return jnp.where(u > -0.35, series, 1.0 - jnp.exp(u))


def soft_plus(u):
    e = jnp.exp(-jnp.abs(u))
    series = jnp.zeros_like(e)
    for k in range(10, 0, -1):
        series = e * (1.0 / k - series)
    return jnp.maximum(u, 0.0) + jnp.where(e < 0.1, series, jnp.log(1.0 + e))


def shifted(value, steps, fill):
    rows = value.shape[0]
    if steps % 8 == 0:
        top = jnp.full((steps, value.shape[1]), fill, value.dtype)
        return jnp.concatenate([top, value[: rows - steps]], axis=0)
    at = lax.broadcasted_iota(jnp.int32, value.shape, 0)
    return jnp.where(at < steps, fill, pltpu.roll(value, steps, 0))


def fused(
    sizes,
    x_hbm,
    branch_w,
    memory_w,
    exit_w,
    taps_hbm,
    reset_hbm,
    inject_hbm,
    forget_hbm,
    mult_hbm,
    spike_hbm,
    gains_hbm,
    final_hbm,
    out_ref,
    x_ref,
    taps_ref,
    reset_w,
    inject_w,
    rate_ref,
    mult_ref,
    spike_ref,
    gains_ref,
    final_ref,
    win,
    wout,
    agx,
    xs,
    nrm,
    nrm_lent,
    ext,
    halo,
    keep_s,
    state_s,
    gel_s,
    mix_s,
    lent_out,
    lent_in,
    part,
    from_sib,
    pair,
    from_far,
    cry_out,
    cry_in,
    hacc,
    mult_s,
    sq_out,
    sq_in,
    sem_load,
    sem_own,
    sem_piece,
    sem_rest,
    sem_w_send,
    sem_lend,
    sem_ag_send,
    sem_ag_recv,
    sem_rs_send,
    sem_rs_recv,
    sem_h,
    sem_c_send,
    sem_c_recv,
    sem_q_send,
    sem_q_recv,
):
    layers, n_sp, n_tp, n_grp, rows, chans, feats, depth, pieces = sizes
    chips = n_tp // 2
    count = 3 * layers
    g, s, t = lax.axis_index("grp"), lax.axis_index("sp"), lax.axis_index("tp")
    core = lax.rem(t, 2)
    chip = t // 2
    sib = chip * 2 + 1 - core
    full = n_tp * feats
    inw = 1 - 2 * (s // (n_sp // 2))
    is_end = (s == 0) | (s == n_sp - 1)
    is_mid = (s > 0) & (s < n_sp - 1)

    def at_end(body):
        pl.when(is_end)(body)

    def at_mid(body):
        pl.when(is_mid)(body)

    width = feats // 2

    def own_half(m, half):
        if m % 3 < 2:
            return (memory_w, branch_w)[m % 3].at[m // 3, half]
        cols = pl.ds(pl.multiple_of(half * width, width), width)
        return exit_w.at[m // 3, :, cols]

    def slot(m, j):
        kind = 2 * (m // 3) + m % 3 if m % 3 < 2 else m // 3
        return (win if m % 3 < 2 else wout), (kind * n_sp + j) * 2

    def keep_half(m, half):
        ref, at = slot(m, s)
        return pltpu.make_async_copy(
            own_half(m, half), ref.at[at + half], sem_own.at[m, half]
        )

    def keep_own(m):
        for half in range(2):
            keep_half(m, half).start()

    def kept(m):
        for half in range(2):
            keep_half(m, half).wait()

    loads = [
        pltpu.make_async_copy(src, dst, sem_load.at[i])
        for i, (src, dst) in enumerate(
            (
                (x_hbm.at[:, 0:width], x_ref.at[0]),
                (x_hbm.at[:, width:], x_ref.at[1]),
                (gains_hbm, gains_ref),
                (mult_hbm, mult_ref),
                (forget_hbm, rate_ref),
                (taps_hbm, taps_ref),
                (reset_hbm, reset_w),
                (inject_hbm, inject_w),
                (spike_hbm, spike_ref),
                (final_hbm, final_ref),
            )
        )
    ]
    barrier = pltpu.get_barrier_semaphore()
    for d in range(1, n_tp):
        pl.semaphore_signal(
            barrier, inc=1, device_id={"tp": lax.rem(t + d, n_tp)}, device_id_type=MESH
        )
    for d in range(1, n_sp):
        pl.semaphore_signal(
            barrier, inc=1, device_id={"sp": lax.rem(s + d, n_sp)}, device_id_type=MESH
        )
    pl.semaphore_signal(barrier, inc=1, device_id={"grp": 1 - g}, device_id_type=MESH)
    for load in loads:
        load.start()
    for m in range(len(LENT), 3 * layers):
        keep_own(m)
    pl.semaphore_wait(barrier, n_tp - 1 + n_sp - 1 + 1)

    IN, OUT, ACROSS = 0, 1, 2

    def target(way):
        if way == ACROSS:
            return {"grp": 1 - g}
        return {"sp": s + inw} if way == IN else {"sp": s - inw}

    def cut(ref, q):
        size = ref.shape[0] // PARTS
        return ref.at[pl.ds(q * size, size)]

    def held(m, j, half, q):
        ref, at = slot(m, j)
        return cut(ref.at[at + half], q)

    def arrival(m, j, place, mine, q):
        away = lax.rem(j - place + 2 * n_sp - 1, n_sp)
        return sem_piece.at[m, away, q] if mine else sem_rest.at[m, away]

    def sent(src, m, j, half, q, way, mine):
        place = s + (inw, -inw, 0)[way]
        return pltpu.make_async_remote_copy(
            src_ref=src,
            dst_ref=held(m, j, half, q),
            send_sem=sem_w_send.at[way],
            recv_sem=arrival(m, j, place, mine, q),
            device_id=target(way),
            device_id_type=MESH,
        )

    def relay(m, j, q, ways):
        src = held(m, j, g, q)
        for way in ways:
            sent(src, m, j, g, q, way, way != ACROSS).start()

    def landed(m, j, q):
        piece = held(m, j, g, q)
        sent(piece, m, j, g, q, ACROSS, True).wait_recv()

    def own(m, way, half, q):
        src = cut(own_half(m, half), q)
        sent(src, m, s, half, q, way, half is g).start()

    def own_both(m, way):
        for q in range(PARTS):
            own(m, way, g, q)

    halves = [(1, g)]
    for m in range(2, count):
        halves += [(m, g), (m - 1, 1 - g)]
    halves.append((count - 1, 1 - g))
    end_line = [(m, half, q) for m, half in halves for q in range(PARTS)]
    mid_in_line = [(m, q) for m in (2, 1, *range(3, count)) for q in range(PARTS)]
    def feed_end(steps):
        steps *= PARTS // 2
        for m, half, q in end_line[:steps]:
            own(m, IN, half, q)
        del end_line[:steps]

    def feed_in(steps):
        for m, q in mid_in_line[:steps]:
            own(m, IN, g, q)
        del mid_in_line[:steps]

    def end_pump(m, i, feed, pieces=range(PARTS)):
        j = s + inw * i
        for q in pieces:
            landed(m, j, q)
            relay(m, j, q, (ACROSS,))
            if q % (PARTS // 2) == PARTS // 2 - 1:
                feed_end(feed)

    def mid_block(k):
        return s + inw * (k if k else -1)

    def mid_ways(m, k):
        if k == 0:
            return (IN,) if m in WHOLE else (IN, ACROSS)
        return (ACROSS,) if m in LENT else (OUT, ACROSS)

    def mid_pump(m, k, feed, pieces=range(PARTS)):
        for q in pieces:
            landed(m, mid_block(k), q)
            relay(m, mid_block(k), q, mid_ways(m, k))
        feed_in(feed)

    def end_do(*acts):
        def body():
            for act in acts:
                act()

        at_end(body)

    def mid_do(*acts):
        def body():
            for act in acts:
                act()

        at_mid(body)

    def E(m, i, feed=0):
        return lambda: end_pump(m, i, feed)

    def M(m, k, feed=0):
        return lambda: mid_pump(m, k, feed)

    def F(steps):
        return lambda: feed_end(steps)

    def ready(m, j):
        ref, at = slot(m, j)
        rest = ref.at[at + 1 - g]
        pltpu.make_async_remote_copy(
            src_ref=rest,
            dst_ref=rest,
            send_sem=sem_w_send.at[ACROSS],
            recv_sem=arrival(m, j, s, False, 0),
            device_id=target(ACROSS),
            device_id_type=MESH,
        ).wait_recv()

    def arrived(m):
        kept(m)
        for d in range(1, n_sp):
            ready(m, lax.rem(s + d, n_sp))

    def wait_sends(way, halves):
        view = win.at[pl.ds(0, halves)]
        pltpu.make_async_remote_copy(
            src_ref=view,
            dst_ref=view,
            send_sem=sem_w_send.at[way],
            recv_sem=sem_rest.at[0, 0],
            device_id=target(ACROSS),
            device_id_type=MESH,
        ).wait_send()

    def close_weights():
        lent, whole = len(LENT), len(WHOLE)

        @at_end
        def _():
            wait_sends(IN, count + whole)
            wait_sends(ACROSS, (count - lent) * (n_sp - 1))

        @at_mid
        def _():
            wait_sends(IN, 2 * count)
            wait_sends(OUT, (count - lent) * (n_sp - 1))
            wait_sends(ACROSS, count * (n_sp - 1) - whole)

    def nth(h):
        return 1 - g if h else g

    def band(ref, h):
        return ref.at[nth(h)]

    def ag_copy(src, layer, owner, h, where):
        return pltpu.make_async_remote_copy(
            src_ref=band(src, h),
            dst_ref=band(agx.at[layer, owner], h),
            send_sem=sem_ag_send.at[layer],
            recv_sem=sem_ag_recv.at[layer, owner, h],
            device_id={"tp": where},
            device_id_type=MESH,
        )

    def ag_start(layer, src, h):
        for d in range(1, chips):
            ag_copy(src, layer, t, h, lax.rem(t + 2 * d, n_tp)).start()
        ag_copy(src, layer, t, h, sib).start()

    def ag_forward(layer):
        for h in range(BANDS):
            for d in range(1, chips):
                owner = lax.rem(t + 2 * d, n_tp)
                block = agx.at[layer, owner]
                ag_copy(block, layer, owner, h, sib).wait_recv()
                ag_copy(block, layer, owner, h, sib).start()

    def ag_finish(layer, src):
        for h in range(BANDS):
            ag_copy(src, layer, sib, h, sib).wait_recv()
            for d in range(1, chips):
                owner = lax.rem(sib + 2 * d, n_tp)
                ag_copy(agx.at[layer, owner], layer, owner, h, sib).wait_recv()

    def wait_blocks(view, sem):
        pltpu.make_async_remote_copy(
            src_ref=view,
            dst_ref=view,
            send_sem=sem,
            recv_sem=sem_rest.at[0, 0],
            device_id=target(ACROSS),
            device_id_type=MESH,
        ).wait_send()

    def ag_close(layer):
        wait_blocks(agx.at[layer, pl.ds(0, 2 * chips - 1)], sem_ag_send.at[layer])

    def lend_rows(h):
        return pltpu.make_async_remote_copy(
            src_ref=band(x_ref, h),
            dst_ref=band(agx.at[layers, t], h),
            send_sem=sem_lend.at[h],
            recv_sem=sem_ag_recv.at[layers, t, h],
            device_id=target(IN),
            device_id_type=MESH,
        )

    def lend_back(i):
        return pltpu.make_async_remote_copy(
            src_ref=lent_out.at[i],
            dst_ref=lent_in.at[i],
            send_sem=sem_lend.at[BANDS + i],
            recv_sem=sem_lend.at[BANDS + len(LENT) + i],
            device_id=target(OUT),
            device_id_type=MESH,
        )

    step = rows // pieces

    def normalize(layer, gain_row, nrm):
        def one(i, carry):
            at = pl.ds(pl.multiple_of(i * step, step), step)
            total = jnp.zeros((step, 1), F32)
            for p in range(n_tp):
                for c in range(2):
                    f = agx[layer, p, c, at].astype(F32)
                    total = total + jnp.sum(f * f, axis=1, keepdims=True)
            inv = lax.rsqrt(total / full + EPSILON)
            for p in range(n_tp):
                for c in range(2):
                    cols = slice(p * feats + c * width, p * feats + (c + 1) * width)
                    f = agx[layer, p, c, at].astype(F32)
                    gain = gains_ref[gain_row : gain_row + 1, cols]
                    nrm[at, cols] = (f * inv * gain).astype(BF16)
            return carry

        lax.fori_loop(0, pieces, one, 0)

    def project(idx, nrm):
        total = None
        for j in range(n_sp):
            at = (idx * n_sp + j) * 2
            term = jnp.dot(
                nrm[:, j * depth : (j + 1) * depth],
                win[at : at + 2].reshape(depth, chans),
                preferred_element_type=F32,
            )
            total = term if total is None else total + term
        return total.astype(BF16)

    def halo_copy(layer):
        return pltpu.make_async_remote_copy(
            src_ref=ext.at[layer, pl.ds(rows, 8)],
            dst_ref=halo.at[layer],
            send_sem=sem_h.at[layer, 0],
            recv_sem=sem_h.at[layer, 1],
            device_id={"sp": s + 1},
            device_id_type=MESH,
        )

    def carry_copy(layer, d):
        return pltpu.make_async_remote_copy(
            src_ref=cry_out.at[layer],
            dst_ref=cry_in.at[layer, s],
            send_sem=sem_c_send.at[layer, d],
            recv_sem=sem_c_recv.at[layer, s],
            device_id={"sp": s + d},
            device_id_type=MESH,
        )

    def carry_wait(layer, j):
        pltpu.make_async_remote_copy(
            src_ref=cry_out.at[layer],
            dst_ref=cry_in.at[layer, j],
            send_sem=sem_c_send.at[layer, 0],
            recv_sem=sem_c_recv.at[layer, j],
            device_id={"sp": s},
            device_id_type=MESH,
        ).wait_recv()

    def rs_copy(src, dst, layer, k, h, where):
        return pltpu.make_async_remote_copy(
            src_ref=src,
            dst_ref=dst,
            send_sem=sem_rs_send.at[layer],
            recv_sem=sem_rs_recv.at[layer, k, h],
            device_id={"tp": where},
            device_id_type=MESH,
        )

    def near_copy(layer, q, h):
        to = lax.rem(sib + 2 * q, n_tp)
        src, dst = band(part.at[layer, to], h), band(from_sib.at[layer, q], h)
        return rs_copy(src, dst, layer, q, h, sib)

    def far_copy(layer, q, h):
        where = lax.rem(t + 2 * q, n_tp)
        src, dst = band(pair.at[layer, q], h), band(from_far.at[layer, q], h)
        return rs_copy(src, dst, layer, chips + q - 1, h, where)

    def first_sender(layer):
        return 1 if layer == 0 else 0

    def send_halo(layer):
        @pl.when((s >= first_sender(layer)) & (s < n_sp - 1))
        def _():
            halo_copy(layer).start()

    def take_halo(layer):
        @pl.when(s == 0)
        def _():
            halo[layer] = jnp.zeros((8, chans), F32)

        if layer == 0:

            @pl.when(s == 1)
            def _():
                halo[layer] = lent_out[0].astype(F32)[rows - 8 :]

        @pl.when(s > first_sender(layer))
        def _():
            halo_copy(layer).wait_recv()

        ext[layer, :8] = halo[layer]

    def gates(layer, b):
        n_taps = taps_ref.shape[1]
        base = 8 - (n_taps - 1)
        cols = slice(b * BLOCK_W, (b + 1) * BLOCK_W)
        conv = jnp.zeros((rows, BLOCK_W), F32)
        for k in range(n_taps):
            tap = taps_ref[layer, k : k + 1, cols].astype(F32)
            conv = conv + ext[layer, base + k : base + k + rows, cols] * tap
        conv = conv.astype(BF16)
        reset = jax.nn.sigmoid(
            jnp.dot(conv, reset_w[layer, b], preferred_element_type=F32)
        )
        inject = jax.nn.sigmoid(
            jnp.dot(conv, inject_w[layer, b], preferred_element_type=F32)
        )
        log_keep = (
            reset * rate_ref[layer : layer + 1, cols] * mult_s[...] + spike_ref[:, cols]
        )
        keep = jnp.exp(log_keep)
        state = inject * conv.astype(F32) * jnp.sqrt(one_minus_exp(2.0 * log_keep))
        lag = 1
        while lag < rows:
            state = keep * shifted(state, lag, 0.0) + state
            keep = keep * shifted(keep, lag, 1.0)
            lag *= 2
        keep_s[:, cols] = keep
        state_s[:, cols] = state
        cry_out[layer, 0:1, cols] = keep[rows - 1 :]
        cry_out[layer, 1:2, cols] = state[rows - 1 :]

    def send_carry(layer):
        for d in range(1, n_sp):

            @pl.when(s + d < n_sp)
            def _():
                carry_copy(layer, d).start()

    def take_carry(layer):
        hacc[...] = jnp.zeros((1, chans), F32)
        for j in range(n_sp - 1):

            @pl.when(j < s)
            def _():
                carry_wait(layer, j)
                hacc[...] = cry_in[layer, j, 0:1] * hacc[...] + cry_in[layer, j, 1:2]

    def mix():
        mix_s[...] = (
            gel_s[...] * (state_s[...] + keep_s[...] * hacc[...])
        ).astype(BF16)

    def chips_on(j):
        return lax.rem(j // 2 - chip + chips, chips)

    def product(layer, j, h):
        half = nth(h)
        part[layer, j, half] = jnp.dot(
            mix_s[...],
            wout[(layer * n_sp + j) * 2 + half],
            preferred_element_type=F32,
        ).astype(BF16)

        @pl.when(lax.rem(j, 2) != core)
        def _():
            near_copy(layer, chips_on(j), h).start()

    def pass_on(layer, j, h):
        q = chips_on(j)
        half = nth(h)

        @pl.when((lax.rem(j, 2) == core) & (q != 0))
        def _():
            near_copy(layer, q, h).wait_recv()
            pair[layer, q, half] = (
                part[layer, j, half].astype(F32) + from_sib[layer, q, half].astype(F32)
            ).astype(BF16)
            far_copy(layer, q, h).start()

    def crossing_order(i):
        there = 2 * (1 - chip) if i < 2 else 2 * chip
        return there + (core if i % 2 else 1 - core)

    def project_out(layer, ahead):
        m = 3 * layer + 2
        e = is_end.astype(jnp.int32)
        turned = (chip == s // (n_tp // chips)).astype(jnp.int32)
        kept(m)

        @at_mid
        def _():
            for d in range(1, n_sp):
                ready(m, lax.rem(s + d, n_sp))

        def place(i):
            step = (0, 1, 2, 3)[i] + turned * (2, -1, -1, 0)[i]
            arriving = s + inw * step
            return step, arriving, crossing_order(i) + e * (arriving - crossing_order(i))

        pair_of = []
        for i in range(2):
            step, arriving, j = place(i)
            ahead(i, 0)
            pl.when(is_end & (step > 0))(functools.partial(ready, m, arriving))
            pair_of.append(j)
        for h in range(BANDS):
            for j in pair_of:
                product(layer, j, h)
            ahead(1, 1 + h)
            for j in pair_of:
                pass_on(layer, j, h)
        for i in range(2, n_sp):
            step, arriving, j = place(i)
            ahead(i, 0)
            product(layer, j, 0)
            ahead(i, 1)
            pass_on(layer, j, 0)
            ahead(i, 2)
            pl.when(is_end & (step > 0))(functools.partial(ready, m, arriving))
            product(layer, j, 1)
            ahead(i, 3)
            pass_on(layer, j, 1)

    def close_layer(layer, src, ahead):
        for h in range(BANDS):
            ahead(h)
            half = nth(h)
            near_copy(layer, 0, h).wait_recv()
            mixed = part[layer, t, half].astype(F32) + from_sib[layer, 0, half].astype(F32)
            for q in range(1, chips):
                far_copy(layer, q, h).wait_recv()
                mixed = mixed + from_far[layer, q, half].astype(F32)
            xs[layer + 1, half] = (src[half].astype(F32) + mixed).astype(BF16)
            if layer + 1 < layers:
                ag_start(layer + 1, xs.at[layer + 1], h)

    own_both(0, IN)
    for load in loads[:2]:
        load.wait()

    @at_end
    def _():
        for h in range(BANDS):
            lend_rows(h).start()
        feed_end(2)

    @at_mid
    def _():
        for h in range(BANDS):
            ag_start(0, x_ref, h)
        for m in range(len(LENT), count - 1):
            own_both(m, OUT)
        for m in LENT:
            keep_own(m)
        agx[0, t] = x_ref[...]

    for load in loads[2:]:
        load.wait()
    rate_ref[...] = -SQUASH_POWER * soft_plus(-rate_ref[...])
    mult_s[...] = jnp.broadcast_to(mult_ref[...].reshape(1, rows), (128, rows)).T[:, 0:1]

    @at_mid
    def _():
        mid_pump(0, 0, PARTS)
        mid_pump(0, 1, 0)
        ag_forward(0)
        ag_finish(0, x_ref)
        normalize(0, 0, nrm)
        lend_rows(0).wait_recv()
        ag_start(layers, agx.at[layers, t], 0)
        mid_pump(0, 2, PARTS)
        for h in range(1, BANDS):
            lend_rows(h).wait_recv()
            ag_start(layers, agx.at[layers, t], h)
        for q in range(PARTS):
            landed(2, mid_block(1), q)
            relay(2, mid_block(1), q, (OUT,))
        own_both(count - 1, OUT)
        ag_forward(layers)
        arrived(0)
        ext[0, 8:] = project(0, nrm).astype(F32)
        send_halo(0)
        for q in range(PARTS):
            landed(1, mid_block(1), q)
            relay(1, mid_block(1), q, mid_ways(1, 1))
            landed(1, mid_block(0), q)
            relay(1, mid_block(0), q, mid_ways(1, 0))
        ag_finish(layers, agx.at[layers, t])
        normalize(layers, 0, nrm_lent)
        lent_out[0] = project(0, nrm_lent)
        lend_back(0).start()
        mid_pump(2, 0, PARTS)
        mid_pump(1, 2, 0)
        for q in range(PARTS):
            relay(2, mid_block(1), q, (ACROSS,))

    @at_end
    def _():
        end_pump(2, 1, 0)
        end_pump(3, 1, 0)
        end_pump(4, 1, 1)
        feed_end(2)
        end_pump(2, 2, 1)
        feed_end(2)
        end_pump(5, 1, 0)
        lend_back(0).wait_recv()
        ext[0, 8:] = lent_in[0].astype(F32)

    take_halo(0)
    gates(0, 0)
    gates(0, 1)
    send_carry(0)

    @at_mid
    def _():
        mid_pump(2, 2, 0, range(PARTS // 2))
        arrived(1)
        lent_out[1] = project(1, nrm_lent)
        lend_back(1).start()
        mid_pump(2, 2, 0, range(PARTS // 2, PARTS))
        gel_s[...] = jax.nn.gelu(project(1, nrm).astype(F32))
        mid_pump(3, 1, 0)
        mid_pump(3, 0, PARTS)

    @at_end
    def _():
        feed_end(4)
        end_pump(2, 3, 0, range(PARTS // 2))
        lend_back(1).wait_recv()
        feed_end(2)
        gel_s[...] = jax.nn.gelu(lent_in[1].astype(F32))

    take_carry(0)
    mix()

    def pieces_of(*runs):
        return [(m, i, q) for m, i, first in runs for q in range(first, PARTS)]

    early = [pieces_of((2, 3, PARTS // 2), (3, 2, 0)) for _ in range(2)]
    final = [pieces_of((4, 3, 0), (5, 2, 0), (5, 3, 0)) for _ in range(2)]

    def end_next(lists, even, odd):
        for parity, steps in ((0, even), (1, odd)):
            now = lists[parity][:steps]
            del lists[parity][:steps]

            @pl.when(is_end & (core == parity))
            def _():
                for m, i, q in now:
                    landed(m, s + inw * i, q)
                    relay(m, s + inw * i, q, (ACROSS,))

    def nothing(_):
        return

    def between(h):
        if h == 0:
            end_do(F(2))
            mid_do(M(3, 2))
        turned = chip == s // (n_tp // chips)
        if h == 0:
            pl.when(is_end & jnp.logical_not(turned))(E(3, 3))
        if h == BANDS - 1:
            pl.when(is_end & turned)(E(3, 3))
            mid_do(M(4, 1), M(4, 0, PARTS))

    def rest_ahead(i, stage):
        even, odd = {
            (1, 0): (0, 1),
            (1, 1): (0, 2),
            (2, 0): (1, 1),
            (3, 0): (1, 0),
            (3, 1): (1, 1),
            (3, 2): (2, 1),
            (3, 3): (1, 0),
        }.get((i, stage), (0, 0))
        end_next(early, even, odd)
        if (i, stage) == (3, 0):
            end_do(F(2))

    project_out(0, rest_ahead)
    close_layer(0, x_ref, between)

    agx[1, t] = xs[1]
    mid_do(M(4, 2), M(5, 0))
    end_do(F(99), E(4, 2))
    end_next(final, 1, 1)
    ag_forward(1)
    end_next(final, 0, 3)
    ag_finish(1, xs.at[1])
    end_next(final, 1, 0)
    normalize(1, 1, nrm)
    end_next(final, 0, 1)
    arrived(3)
    ext[1, 8:] = project(2, nrm).astype(F32)
    send_halo(1)
    mid_do(M(5, 1))
    pl.when(s == 1)(M(5, 2))
    end_next(final, 1, 1)
    take_halo(1)
    gates(1, 0)
    end_next(final, 1, 1)
    gates(1, 1)
    send_carry(1)
    pl.when(is_mid & (s > 1))(M(5, 2))
    end_next(final, 2, 1)
    arrived(4)
    end_next(final, 1, 0)
    gel_s[...] = jax.nn.gelu(project(3, nrm).astype(F32))
    end_next(final, 2, 2)
    take_carry(1)
    mix()

    def last_ahead(i, stage):
        even, odd = {(0, 0): (1, 2), (1, 1): (1, 0), (2, 0): (1, 0)}.get((i, stage), (0, 0))
        end_next(final, even, odd)

    project_out(1, last_ahead)
    close_layer(1, xs.at[1], nothing)

    square = jnp.zeros((rows, 1), F32)
    for c in range(2):
        fresh = xs[layers, c].astype(F32)
        square = square + jnp.sum(fresh * fresh, axis=1, keepdims=True)
    sq_out[...] = jnp.broadcast_to(square, (rows, 128)).T[0:8]

    def sq_copy(d):
        return pltpu.make_async_remote_copy(
            src_ref=sq_out,
            dst_ref=sq_in.at[d],
            send_sem=sem_q_send.at[d],
            recv_sem=sem_q_recv.at[d],
            device_id={"tp": lax.rem(t + d, n_tp)},
            device_id_type=MESH,
        )

    for d in range(1, n_tp):
        sq_copy(d).start()
    total = sq_out[0:1]
    for d in range(1, n_tp):
        sq_copy(d).wait_recv()
        total = total + sq_in[d, 0:1]
    inv = lax.rsqrt(total / full + EPSILON)
    inv = jnp.broadcast_to(inv, (128, rows)).T[:, 0:1]
    for c in range(2):
        cols = slice(c * width, (c + 1) * width)
        fresh = xs[layers, c].astype(F32)
        out_ref[:, cols] = (fresh * inv * final_ref[:, cols]).astype(BF16)

    assert not (end_line or mid_in_line or any(early) or any(final))
    close_weights()

    @at_end
    def _():
        for h in range(BANDS):
            lend_rows(h).wait_send()

    @at_mid
    def _():
        ag_close(0)
        ag_close(layers)
        for i in range(len(LENT)):
            lend_back(i).wait_send()

    for layer in range(layers):
        if layer:
            ag_close(layer)

        @pl.when((s >= first_sender(layer)) & (s < n_sp - 1))
        def _():
            halo_copy(layer).wait_send()

        for d in range(1, n_sp):

            @pl.when(s + d < n_sp)
            def _():
                carry_copy(layer, d).wait_send()

        wait_blocks(part.at[layer, pl.ds(0, 2 * chips - 1)], sem_rs_send.at[layer])
    for d in range(1, n_tp):
        sq_copy(d).wait_send()


def in_one_kernel(
    sizes_of,
    starting_stream,
    multiplier_matrix,
    memory_path_matrix,
    filter_coefficients,
    memory_valve_matrix,
    entry_valve_matrix,
    forgetting_parameters,
    timestep_forgetting_multiplier,
    spike_extra,
    exit_projector_matrix,
    prelude_rms_gains,
    finishing_rms_gains,
):
    n_grp, n_sp, n_tp = sizes_of
    rows, feats = starting_stream.shape
    layers, depth, chans = memory_path_matrix.shape
    pieces = rows // 128 if rows % 128 == 0 else 1
    sizes = (layers, n_sp, n_tp, n_grp, rows, chans, feats, depth, pieces)
    chips = n_tp // 2
    half_in = (layers, 2, depth // 2, chans)
    vmem = pl.BlockSpec(memory_space=pltpu.VMEM)
    hbm = pl.BlockSpec(memory_space=pl.ANY)
    count = 3 * layers
    dma = pltpu.SemaphoreType.DMA
    return pl.pallas_call(
        functools.partial(fused, sizes),
        out_shape=jax.ShapeDtypeStruct((rows, feats), BF16),
        in_specs=[hbm] * 12,
        out_specs=vmem,
        scratch_shapes=[
            pltpu.VMEM((2, rows, feats // 2), BF16),
            pltpu.VMEM(filter_coefficients.shape, BF16),
            pltpu.VMEM(memory_valve_matrix.shape, BF16),
            pltpu.VMEM(entry_valve_matrix.shape, BF16),
            pltpu.VMEM((layers, chans), F32),
            pltpu.VMEM((rows,), F32),
            pltpu.VMEM((rows, chans), F32),
            pltpu.VMEM((layers, n_tp * feats), F32),
            pltpu.VMEM((1, feats), F32),
            pltpu.VMEM((2 * layers * n_sp * 2, depth // 2, chans), BF16),
            pltpu.VMEM((layers * n_sp * 2, chans, depth // 2), BF16),
            pltpu.VMEM((layers + 1, n_tp, 2, rows, feats // 2), BF16),
            pltpu.VMEM((layers + 1, 2, rows, feats // 2), BF16),
            pltpu.VMEM((rows, n_tp * feats), BF16),
            pltpu.VMEM((rows, n_tp * feats), BF16),
            pltpu.VMEM((layers, 8 + rows, chans), F32),
            pltpu.VMEM((layers, 8, chans), F32),
            pltpu.VMEM((rows, chans), F32),
            pltpu.VMEM((rows, chans), F32),
            pltpu.VMEM((rows, chans), F32),
            pltpu.VMEM((rows, chans), BF16),
            pltpu.VMEM((len(LENT), rows, chans), BF16),
            pltpu.VMEM((len(LENT), rows, chans), BF16),
            pltpu.VMEM((layers, n_tp, 2, rows, feats // 2), BF16),
            pltpu.VMEM((layers, chips, 2, rows, feats // 2), BF16),
            pltpu.VMEM((layers, chips, 2, rows, feats // 2), BF16),
            pltpu.VMEM((layers, chips, 2, rows, feats // 2), BF16),
            pltpu.VMEM((layers, 2, chans), F32),
            pltpu.VMEM((layers, n_sp, 2, chans), F32),
            pltpu.VMEM((1, chans), F32),
            pltpu.VMEM((rows, 1), F32),
            pltpu.VMEM((8, rows), F32),
            pltpu.VMEM((n_tp, 8, rows), F32),
            dma((10,)),
            dma((count, 2)),
            dma((count, n_sp - 1, PARTS)),
            dma((count, n_sp - 1)),
            dma((3,)),
            dma((BANDS + 2 * len(LENT),)),
            dma((layers + 1,)),
            dma((layers + 1, n_tp, BANDS)),
            dma((layers,)),
            dma((layers, 2 * chips - 1, BANDS)),
            dma((layers, 2)),
            dma((layers, n_sp)),
            dma((layers, n_sp)),
            dma((n_tp,)),
            dma((n_tp,)),
        ],
        compiler_params=pltpu.CompilerParams(
            collective_id=0, has_side_effects=True, vmem_limit_bytes=60 * 2**20
        ),
    )(
        starting_stream,
        multiplier_matrix.reshape(half_in),
        memory_path_matrix.reshape(half_in),
        exit_projector_matrix,
        filter_coefficients,
        memory_valve_matrix,
        entry_valve_matrix,
        forgetting_parameters,
        timestep_forgetting_multiplier,
        spike_extra,
        prelude_rms_gains,
        finishing_rms_gains.reshape(1, feats),
    )


def on_each(sizes_of, *arrays):
    stream, memory = arrays[0], arrays[2]
    n_grp, n_sp, n_tp = sizes_of
    rows, feats = stream.shape
    depth, chans = memory.shape[1:]
    fits = (
        n_grp == 2
        and n_sp == 4
        and memory.shape[0] == 2
        and n_tp % 2 == 0
        and rows % 128 == 0
        and depth % 128 == 0
        and feats % 256 == 0
        and chans % BLOCK_W == 0
        and depth == feats
        and n_sp == n_tp
    )
    if fits:
        return in_one_kernel(sizes_of, *arrays)
    return on_device(*arrays)


def solution(mesh):
    sizes_of = tuple(mesh.shape[axis] for axis in ("grp", "sp", "tp"))
    body = functools.partial(on_each, sizes_of)
    return jax.shard_map(
        body,
        mesh=mesh,
        in_specs=(
            P(("grp", "sp"), "tp"),
            P(None, "sp", "tp"),
            P(None, "sp", "tp"),
            P(None, None, "tp"),
            P(None, "tp", None, None),
            P(None, "tp", None, None),
            P(None, "tp"),
            P(("grp", "sp")),
            P(("grp", "sp"), "tp"),
            P(None, "tp", "sp"),
            P(),
            P("tp"),
        ),
        out_specs=P(("grp", "sp"), "tp"),
        check_vma=False,
    )
```

```python
import functools

import jax
import jax.numpy as jnp
from jax import lax
from jax.experimental import pallas as pl
from jax.experimental.pallas import tpu as pltpu
from jax.sharding import PartitionSpec as P

BLOCK_W = 256


EPSILON = 1e-06
SQUASH_POWER = 8.0


def from_behind(value, axis, steps):
    count = lax.axis_size(axis)
    first, last = (max(0, -steps), min(count, count - steps))
    return lax.ppermute(value, axis, [(source, source + steps) for source in range(first, last)])


def entering(part, axis, combine, identity):
    place = lax.axis_index(axis)
    gathered = jax.tree.map(lambda a: lax.all_gather(a, axis), part)
    state = jax.tree.map(lambda a, e: jnp.zeros_like(a) + jnp.asarray(e, a.dtype), part, identity)

    def one(lap, state):
        return combine(
            state, jax.tree.map(lambda a: lax.dynamic_index_in_dim(a, lap, 0, False), gathered)
        )

    return lax.fori_loop(0, place, one, state)


def combine_pairs(earlier, later):
    return (earlier[0] * later[0], later[0] * earlier[1] + later[1])


def gather_rows(own_cols):
    return lax.all_gather(own_cols, "tp", axis=1, tiled=True)


def on_device(
    starting_stream,
    multiplier_matrix,
    memory_path_matrix,
    filter_coefficients,
    memory_valve_matrix,
    entry_valve_matrix,
    forgetting_parameters,
    timestep_forgetting_multiplier,
    spike_extra,
    exit_projector_matrix,
    prelude_rms_gains,
    finishing_rms_gains,
):
    tok_rows = starting_stream.shape[0]
    channels = memory_path_matrix.shape[2]
    own_cols = starting_stream
    full_rows = gather_rows(starting_stream)
    for tier_number in range(memory_path_matrix.shape[0]):
        floats = full_rows.astype(jnp.float32)
        mean_square = jnp.mean(floats * floats, axis=1, keepdims=True)
        normed = (
            floats * lax.rsqrt(mean_square + EPSILON) * prelude_rms_gains[tier_number][None, :]
        ).astype(jnp.bfloat16)
        branch_acc = jnp.dot(
            normed,
            lax.all_gather(multiplier_matrix[tier_number], "sp", axis=0, tiled=True),
            preferred_element_type=jnp.float32,
        )
        recur_acc = jnp.dot(
            normed,
            lax.all_gather(memory_path_matrix[tier_number], "sp", axis=0, tiled=True),
            preferred_element_type=jnp.float32,
        )
        branch = branch_acc.astype(jnp.bfloat16)
        recurrent = recur_acc.astype(jnp.bfloat16)
        taps_now = filter_coefficients[tier_number]
        reach_back = taps_now.shape[0] - 1
        halo_rows = from_behind(recurrent[tok_rows - reach_back :], "sp", 1)
        extended = jnp.concatenate([halo_rows, recurrent], axis=0)
        conv_sum = jnp.zeros((tok_rows, channels), jnp.float32)
        for offset in range(taps_now.shape[0]):
            conv_sum = conv_sum + extended[offset : offset + tok_rows].astype(
                jnp.float32
            ) * taps_now[offset].astype(jnp.float32)
        convolved = conv_sum.astype(jnp.bfloat16)
        blocks = convolved.reshape(tok_rows, channels // BLOCK_W, BLOCK_W)
        reset_gate = jax.nn.sigmoid(
            jnp.einsum(
                "tnc,ncd->tnd",
                blocks,
                memory_valve_matrix[tier_number],
                preferred_element_type=jnp.float32,
            ).reshape(tok_rows, channels)
        )
        inject = jax.nn.sigmoid(
            jnp.einsum(
                "tnc,ncd->tnd",
                blocks,
                entry_valve_matrix[tier_number],
                preferred_element_type=jnp.float32,
            ).reshape(tok_rows, channels)
        )
        logarithmic_persistence = (
            -SQUASH_POWER
            * reset_gate
            * jax.nn.softplus(-forgetting_parameters[tier_number])[None, :]
            * timestep_forgetting_multiplier[:, None]
            + spike_extra
        )
        keep_rate = jnp.exp(logarithmic_persistence)
        driven = (
            inject
            * convolved.astype(jnp.float32)
            * jnp.sqrt(-jnp.expm1(2.0 * logarithmic_persistence))
        )
        keep_cum, state_local = lax.associative_scan(combine_pairs, (keep_rate, driven), axis=0)
        identity = (jnp.ones((channels,), jnp.float32), jnp.zeros((channels,), jnp.float32))
        carried = entering((keep_cum[-1], state_local[-1]), "sp", combine_pairs, identity)
        state_seq = state_local + keep_cum * carried[1][None, :]
        mixed_in = (jax.nn.gelu(branch.astype(jnp.float32)) * state_seq).astype(jnp.bfloat16)
        partial_value = jnp.dot(
            mixed_in,
            lax.all_gather(exit_projector_matrix[tier_number], "sp", axis=1, tiled=True),
            preferred_element_type=jnp.float32,
        )
        mixed_sum = lax.psum_scatter(
            partial_value.astype(jnp.bfloat16), "tp", scatter_dimension=1, tiled=True
        ).astype(jnp.float32)
        own_cols = (own_cols.astype(jnp.float32) + mixed_sum).astype(jnp.bfloat16)
        if tier_number + 1 < memory_path_matrix.shape[0]:
            full_rows = gather_rows(own_cols)
    floats = own_cols.astype(jnp.float32)
    full_width = floats.shape[1] * lax.axis_size("tp")
    square_sum = lax.psum(jnp.sum(floats * floats, axis=1), "tp")
    inv_rms = lax.rsqrt(square_sum / full_width + EPSILON)
    return (floats * inv_rms[:, None] * finishing_rms_gains[None, :]).astype(jnp.bfloat16)


MESH = pl.DeviceIdType.MESH
F32, BF16 = jnp.float32, jnp.bfloat16

PARTS = 4
BANDS = 2
LENT = (0, 1)
WHOLE = (1, 2, 3, 4, 5)


def one_minus_exp(u):
    series = -u * (
        1 + u / 2 * (1 + u / 3 * (1 + u / 4 * (1 + u / 5 * (1 + u / 6 * (1 + u / 7)))))
    )
    return jnp.where(u > -0.35, series, 1.0 - jnp.exp(u))


def soft_plus(u):
    e = jnp.exp(-jnp.abs(u))
    series = jnp.zeros_like(e)
    for k in range(10, 0, -1):
        series = e * (1.0 / k - series)
    return jnp.maximum(u, 0.0) + jnp.where(e < 0.1, series, jnp.log(1.0 + e))


def shifted(value, steps, fill):
    rows = value.shape[0]
    if steps % 8 == 0:
        top = jnp.full((steps, value.shape[1]), fill, value.dtype)
        return jnp.concatenate([top, value[: rows - steps]], axis=0)
    at = lax.broadcasted_iota(jnp.int32, value.shape, 0)
    return jnp.where(at < steps, fill, pltpu.roll(value, steps, 0))


def fused(
    sizes,
    x_hbm,
    branch_w,
    memory_w,
    exit_w,
    taps_hbm,
    reset_hbm,
    inject_hbm,
    forget_hbm,
    mult_hbm,
    spike_hbm,
    gains_hbm,
    final_hbm,
    out_ref,
    x_ref,
    taps_ref,
    reset_w,
    inject_w,
    rate_ref,
    mult_ref,
    spike_ref,
    gains_ref,
    final_ref,
    win,
    wout,
    agx,
    xs,
    nrm,
    nrm_lent,
    ext,
    halo,
    keep_s,
    state_s,
    gel_s,
    mix_s,
    lent_out,
    lent_in,
    part,
    from_sib,
    pair,
    from_far,
    cry_out,
    cry_in,
    hacc,
    mult_s,
    sq_out,
    sq_in,
    sem_load,
    sem_own,
    sem_piece,
    sem_rest,
    sem_w_send,
    sem_lend,
    sem_ag_send,
    sem_ag_recv,
    sem_rs_send,
    sem_rs_recv,
    sem_h,
    sem_c_send,
    sem_c_recv,
    sem_q_send,
    sem_q_recv,
):
    layers, n_sp, n_tp, n_grp, rows, chans, feats, depth, pieces = sizes
    chips = n_tp // 2
    count = 3 * layers
    g, s, t = lax.axis_index("grp"), lax.axis_index("sp"), lax.axis_index("tp")
    core = lax.rem(t, 2)
    chip = t // 2
    sib = chip * 2 + 1 - core
    full = n_tp * feats
    inw = 1 - 2 * (s // (n_sp // 2))
    is_end = (s == 0) | (s == n_sp - 1)
    is_mid = (s > 0) & (s < n_sp - 1)

    def at_end(body):
        pl.when(is_end)(body)

    def at_mid(body):
        pl.when(is_mid)(body)

    width = feats // 2

    def own_half(m, half):
        if m % 3 < 2:
            return (memory_w, branch_w)[m % 3].at[m // 3, half]
        cols = pl.ds(pl.multiple_of(half * width, width), width)
        return exit_w.at[m // 3, :, cols]

    def slot(m, j):
        kind = 2 * (m // 3) + m % 3 if m % 3 < 2 else m // 3
        return (win if m % 3 < 2 else wout), (kind * n_sp + j) * 2

    def keep_half(m, half):
        ref, at = slot(m, s)
        return pltpu.make_async_copy(
            own_half(m, half), ref.at[at + half], sem_own.at[m, half]
        )

    def keep_own(m):
        for half in range(2):
            keep_half(m, half).start()

    def kept(m):
        for half in range(2):
            keep_half(m, half).wait()

    loads = [
        pltpu.make_async_copy(src, dst, sem_load.at[i])
        for i, (src, dst) in enumerate(
            (
                (x_hbm.at[:, 0:width], x_ref.at[0]),
                (x_hbm.at[:, width:], x_ref.at[1]),
                (gains_hbm, gains_ref),
                (mult_hbm, mult_ref),
                (forget_hbm, rate_ref),
                (taps_hbm, taps_ref),
                (reset_hbm, reset_w),
                (inject_hbm, inject_w),
                (spike_hbm, spike_ref),
                (final_hbm, final_ref),
            )
        )
    ]
    barrier = pltpu.get_barrier_semaphore()
    for d in range(1, n_tp):
        pl.semaphore_signal(
            barrier, inc=1, device_id={"tp": lax.rem(t + d, n_tp)}, device_id_type=MESH
        )
    for d in range(1, n_sp):
        pl.semaphore_signal(
            barrier, inc=1, device_id={"sp": lax.rem(s + d, n_sp)}, device_id_type=MESH
        )
    pl.semaphore_signal(barrier, inc=1, device_id={"grp": 1 - g}, device_id_type=MESH)
    for load in loads:
        load.start()
    for m in range(len(LENT), 3 * layers):
        keep_own(m)
    pl.semaphore_wait(barrier, n_tp - 1 + n_sp - 1 + 1)

    IN, OUT, ACROSS = 0, 1, 2

    def target(way):
        if way == ACROSS:
            return {"grp": 1 - g}
        return {"sp": s + inw} if way == IN else {"sp": s - inw}

    def cut(ref, q):
        size = ref.shape[0] // PARTS
        return ref.at[pl.ds(q * size, size)]

    def held(m, j, half, q):
        ref, at = slot(m, j)
        return cut(ref.at[at + half], q)

    def arrival(m, j, place, mine, q):
        away = lax.rem(j - place + 2 * n_sp - 1, n_sp)
        return sem_piece.at[m, away, q] if mine else sem_rest.at[m, away]

    def sent(src, m, j, half, q, way, mine):
        place = s + (inw, -inw, 0)[way]
        return pltpu.make_async_remote_copy(
            src_ref=src,
            dst_ref=held(m, j, half, q),
            send_sem=sem_w_send.at[way],
            recv_sem=arrival(m, j, place, mine, q),
            device_id=target(way),
            device_id_type=MESH,
        )

    def relay(m, j, q, ways):
        src = held(m, j, g, q)
        for way in ways:
            sent(src, m, j, g, q, way, way != ACROSS).start()

    def landed(m, j, q):
        piece = held(m, j, g, q)
        sent(piece, m, j, g, q, ACROSS, True).wait_recv()

    def own(m, way, half, q):
        src = cut(own_half(m, half), q)
        sent(src, m, s, half, q, way, half is g).start()

    def own_both(m, way):
        for q in range(PARTS):
            own(m, way, g, q)

    halves = [(1, g)]
    for m in range(2, count):
        halves += [(m, g), (m - 1, 1 - g)]
    halves.append((count - 1, 1 - g))
    end_line = [(m, half, q) for m, half in halves for q in range(PARTS)]
    mid_in_line = [(m, q) for m in (2, 1, *range(3, count)) for q in range(PARTS)]
    def feed_end(steps):
        steps *= PARTS // 2
        for m, half, q in end_line[:steps]:
            own(m, IN, half, q)
        del end_line[:steps]

    def feed_in(steps):
        for m, q in mid_in_line[:steps]:
            own(m, IN, g, q)
        del mid_in_line[:steps]

    def end_pump(m, i, feed, pieces=range(PARTS)):
        j = s + inw * i
        for q in pieces:
            landed(m, j, q)
            relay(m, j, q, (ACROSS,))
            if q % (PARTS // 2) == PARTS // 2 - 1:
                feed_end(feed)

    def mid_block(k):
        return s + inw * (k if k else -1)

    def mid_ways(m, k):
        if k == 0:
            return (IN,) if m in WHOLE else (IN, ACROSS)
        return (ACROSS,) if m in LENT else (OUT, ACROSS)

    def mid_pump(m, k, feed, pieces=range(PARTS)):
        for q in pieces:
            landed(m, mid_block(k), q)
            relay(m, mid_block(k), q, mid_ways(m, k))
        feed_in(feed)

    def end_do(*acts):
        def body():
            for act in acts:
                act()

        at_end(body)

    def mid_do(*acts):
        def body():
            for act in acts:
                act()

        at_mid(body)

    def E(m, i, feed=0):
        return lambda: end_pump(m, i, feed)

    def M(m, k, feed=0):
        return lambda: mid_pump(m, k, feed)

    def F(steps):
        return lambda: feed_end(steps)

    def ready(m, j):
        ref, at = slot(m, j)
        rest = ref.at[at + 1 - g]
        pltpu.make_async_remote_copy(
            src_ref=rest,
            dst_ref=rest,
            send_sem=sem_w_send.at[ACROSS],
            recv_sem=arrival(m, j, s, False, 0),
            device_id=target(ACROSS),
            device_id_type=MESH,
        ).wait_recv()

    def arrived(m):
        kept(m)
        for d in range(1, n_sp):
            ready(m, lax.rem(s + d, n_sp))

    def wait_sends(way, halves):
        view = win.at[pl.ds(0, halves)]
        pltpu.make_async_remote_copy(
            src_ref=view,
            dst_ref=view,
            send_sem=sem_w_send.at[way],
            recv_sem=sem_rest.at[0, 0],
            device_id=target(ACROSS),
            device_id_type=MESH,
        ).wait_send()

    def close_weights():
        lent, whole = len(LENT), len(WHOLE)

        @at_end
        def _():
            wait_sends(IN, count + whole)
            wait_sends(ACROSS, (count - lent) * (n_sp - 1))

        @at_mid
        def _():
            wait_sends(IN, 2 * count)
            wait_sends(OUT, (count - lent) * (n_sp - 1))
            wait_sends(ACROSS, count * (n_sp - 1) - whole)

    def nth(h):
        return 1 - g if h else g

    def band(ref, h):
        return ref.at[nth(h)]

    def ag_copy(src, layer, owner, h, where):
        return pltpu.make_async_remote_copy(
            src_ref=band(src, h),
            dst_ref=band(agx.at[layer, owner], h),
            send_sem=sem_ag_send.at[layer],
            recv_sem=sem_ag_recv.at[layer, owner, h],
            device_id={"tp": where},
            device_id_type=MESH,
        )

    def ag_start(layer, src, h):
        for d in range(1, chips):
            ag_copy(src, layer, t, h, lax.rem(t + 2 * d, n_tp)).start()
        ag_copy(src, layer, t, h, sib).start()

    def ag_forward(layer):
        for h in range(BANDS):
            for d in range(1, chips):
                owner = lax.rem(t + 2 * d, n_tp)
                block = agx.at[layer, owner]
                ag_copy(block, layer, owner, h, sib).wait_recv()
                ag_copy(block, layer, owner, h, sib).start()

    def ag_finish(layer, src):
        for h in range(BANDS):
            ag_copy(src, layer, sib, h, sib).wait_recv()
            for d in range(1, chips):
                owner = lax.rem(sib + 2 * d, n_tp)
                ag_copy(agx.at[layer, owner], layer, owner, h, sib).wait_recv()

    def wait_blocks(view, sem):
        pltpu.make_async_remote_copy(
            src_ref=view,
            dst_ref=view,
            send_sem=sem,
            recv_sem=sem_rest.at[0, 0],
            device_id=target(ACROSS),
            device_id_type=MESH,
        ).wait_send()

    def ag_close(layer):
        wait_blocks(agx.at[layer, pl.ds(0, 2 * chips - 1)], sem_ag_send.at[layer])

    def lend_rows(h):
        return pltpu.make_async_remote_copy(
            src_ref=band(x_ref, h),
            dst_ref=band(agx.at[layers, t], h),
            send_sem=sem_lend.at[h],
            recv_sem=sem_ag_recv.at[layers, t, h],
            device_id=target(IN),
            device_id_type=MESH,
        )

    def lend_back(i):
        return pltpu.make_async_remote_copy(
            src_ref=lent_out.at[i],
            dst_ref=lent_in.at[i],
            send_sem=sem_lend.at[BANDS + i],
            recv_sem=sem_lend.at[BANDS + len(LENT) + i],
            device_id=target(OUT),
            device_id_type=MESH,
        )

    step = rows // pieces

    def normalize(layer, gain_row, nrm):
        def one(i, carry):
            at = pl.ds(pl.multiple_of(i * step, step), step)
            total = jnp.zeros((step, 1), F32)
            for p in range(n_tp):
                for c in range(2):
                    f = agx[layer, p, c, at].astype(F32)
                    total = total + jnp.sum(f * f, axis=1, keepdims=True)
            inv = lax.rsqrt(total / full + EPSILON)
            for p in range(n_tp):
                for c in range(2):
                    cols = slice(p * feats + c * width, p * feats + (c + 1) * width)
                    f = agx[layer, p, c, at].astype(F32)
                    gain = gains_ref[gain_row : gain_row + 1, cols]
                    nrm[at, cols] = (f * inv * gain).astype(BF16)
            return carry

        lax.fori_loop(0, pieces, one, 0)

    def project(idx, nrm):
        total = None
        for j in range(n_sp):
            at = (idx * n_sp + j) * 2
            term = jnp.dot(
                nrm[:, j * depth : (j + 1) * depth],
                win[at : at + 2].reshape(depth, chans),
                preferred_element_type=F32,
            )
            total = term if total is None else total + term
        return total.astype(BF16)

    def halo_copy(layer):
        return pltpu.make_async_remote_copy(
            src_ref=ext.at[layer, pl.ds(rows, 8)],
            dst_ref=halo.at[layer],
            send_sem=sem_h.at[layer, 0],
            recv_sem=sem_h.at[layer, 1],
            device_id={"sp": s + 1},
            device_id_type=MESH,
        )

    def carry_copy(layer, d):
        return pltpu.make_async_remote_copy(
            src_ref=cry_out.at[layer],
            dst_ref=cry_in.at[layer, s],
            send_sem=sem_c_send.at[layer, d],
            recv_sem=sem_c_recv.at[layer, s],
            device_id={"sp": s + d},
            device_id_type=MESH,
        )

    def carry_wait(layer, j):
        pltpu.make_async_remote_copy(
            src_ref=cry_out.at[layer],
            dst_ref=cry_in.at[layer, j],
            send_sem=sem_c_send.at[layer, 0],
            recv_sem=sem_c_recv.at[layer, j],
            device_id={"sp": s},
            device_id_type=MESH,
        ).wait_recv()

    def rs_copy(src, dst, layer, k, h, where):
        return pltpu.make_async_remote_copy(
            src_ref=src,
            dst_ref=dst,
            send_sem=sem_rs_send.at[layer],
            recv_sem=sem_rs_recv.at[layer, k, h],
            device_id={"tp": where},
            device_id_type=MESH,
        )

    def near_copy(layer, q, h):
        to = lax.rem(sib + 2 * q, n_tp)
        src, dst = band(part.at[layer, to], h), band(from_sib.at[layer, q], h)
        return rs_copy(src, dst, layer, q, h, sib)

    def far_copy(layer, q, h):
        where = lax.rem(t + 2 * q, n_tp)
        src, dst = band(pair.at[layer, q], h), band(from_far.at[layer, q], h)
        return rs_copy(src, dst, layer, chips + q - 1, h, where)

    def first_sender(layer):
        return 1 if layer == 0 else 0

    def send_halo(layer):
        @pl.when((s >= first_sender(layer)) & (s < n_sp - 1))
        def _():
            halo_copy(layer).start()

    def take_halo(layer):
        @pl.when(s == 0)
        def _():
            halo[layer] = jnp.zeros((8, chans), F32)

        if layer == 0:

            @pl.when(s == 1)
            def _():
                halo[layer] = lent_out[0].astype(F32)[rows - 8 :]

        @pl.when(s > first_sender(layer))
        def _():
            halo_copy(layer).wait_recv()

        ext[layer, :8] = halo[layer]

    def gates(layer, b):
        n_taps = taps_ref.shape[1]
        base = 8 - (n_taps - 1)
        cols = slice(b * BLOCK_W, (b + 1) * BLOCK_W)
        conv = jnp.zeros((rows, BLOCK_W), F32)
        for k in range(n_taps):
            tap = taps_ref[layer, k : k + 1, cols].astype(F32)
            conv = conv + ext[layer, base + k : base + k + rows, cols] * tap
        conv = conv.astype(BF16)
        reset = jax.nn.sigmoid(
            jnp.dot(conv, reset_w[layer, b], preferred_element_type=F32)
        )
        inject = jax.nn.sigmoid(
            jnp.dot(conv, inject_w[layer, b], preferred_element_type=F32)
        )
        log_keep = (
            reset * rate_ref[layer : layer + 1, cols] * mult_s[...] + spike_ref[:, cols]
        )
        keep = jnp.exp(log_keep)
        state = inject * conv.astype(F32) * jnp.sqrt(one_minus_exp(2.0 * log_keep))
        lag = 1
        while lag < rows:
            state = keep * shifted(state, lag, 0.0) + state
            keep = keep * shifted(keep, lag, 1.0)
            lag *= 2
        keep_s[:, cols] = keep
        state_s[:, cols] = state
        cry_out[layer, 0:1, cols] = keep[rows - 1 :]
        cry_out[layer, 1:2, cols] = state[rows - 1 :]

    def send_carry(layer):
        for d in range(1, n_sp):

            @pl.when(s + d < n_sp)
            def _():
                carry_copy(layer, d).start()

    def take_carry(layer):
        hacc[...] = jnp.zeros((1, chans), F32)
        for j in range(n_sp - 1):

            @pl.when(j < s)
            def _():
                carry_wait(layer, j)
                hacc[...] = cry_in[layer, j, 0:1] * hacc[...] + cry_in[layer, j, 1:2]

    def mix():
        mix_s[...] = (
            gel_s[...] * (state_s[...] + keep_s[...] * hacc[...])
        ).astype(BF16)

    def chips_on(j):
        return lax.rem(j // 2 - chip + chips, chips)

    def product(layer, j, h):
        half = nth(h)
        part[layer, j, half] = jnp.dot(
            mix_s[...],
            wout[(layer * n_sp + j) * 2 + half],
            preferred_element_type=F32,
        ).astype(BF16)

        @pl.when(lax.rem(j, 2) != core)
        def _():
            near_copy(layer, chips_on(j), h).start()

    def pass_on(layer, j, h):
        q = chips_on(j)
        half = nth(h)

        @pl.when((lax.rem(j, 2) == core) & (q != 0))
        def _():
            near_copy(layer, q, h).wait_recv()
            pair[layer, q, half] = (
                part[layer, j, half].astype(F32) + from_sib[layer, q, half].astype(F32)
            ).astype(BF16)
            far_copy(layer, q, h).start()

    def crossing_order(i):
        there = 2 * (1 - chip) if i < 2 else 2 * chip
        return there + (core if i % 2 else 1 - core)

    def project_out(layer, ahead):
        m = 3 * layer + 2
        e = is_end.astype(jnp.int32)
        turned = (chip == s // (n_tp // chips)).astype(jnp.int32)
        kept(m)

        @at_mid
        def _():
            for d in range(1, n_sp):
                ready(m, lax.rem(s + d, n_sp))

        def place(i):
            step = (0, 1, 2, 3)[i] + turned * (2, -1, -1, 0)[i]
            arriving = s + inw * step
            return step, arriving, crossing_order(i) + e * (arriving - crossing_order(i))

        pair_of = []
        for i in range(2):
            step, arriving, j = place(i)
            ahead(i, 0)
            pl.when(is_end & (step > 0))(functools.partial(ready, m, arriving))
            pair_of.append(j)
        for h in range(BANDS):
            for j in pair_of:
                product(layer, j, h)
            ahead(1, 1 + h)
            for j in pair_of:
                pass_on(layer, j, h)
        for i in range(2, n_sp):
            step, arriving, j = place(i)
            ahead(i, 0)
            product(layer, j, 0)
            ahead(i, 1)
            pass_on(layer, j, 0)
            ahead(i, 2)
            pl.when(is_end & (step > 0))(functools.partial(ready, m, arriving))
            product(layer, j, 1)
            ahead(i, 3)
            pass_on(layer, j, 1)

    def close_layer(layer, src, ahead):
        for h in range(BANDS):
            ahead(h)
            half = nth(h)
            near_copy(layer, 0, h).wait_recv()
            mixed = part[layer, t, half].astype(F32) + from_sib[layer, 0, half].astype(F32)
            for q in range(1, chips):
                far_copy(layer, q, h).wait_recv()
                mixed = mixed + from_far[layer, q, half].astype(F32)
            xs[layer + 1, half] = (src[half].astype(F32) + mixed).astype(BF16)
            if layer + 1 < layers:
                ag_start(layer + 1, xs.at[layer + 1], h)

    own_both(0, IN)
    for load in loads[:2]:
        load.wait()

    @at_end
    def _():
        for h in range(BANDS):
            lend_rows(h).start()
        feed_end(2)

    @at_mid
    def _():
        for h in range(BANDS):
            ag_start(0, x_ref, h)
        for m in range(len(LENT), count - 1):
            own_both(m, OUT)
        for m in LENT:
            keep_own(m)
        agx[0, t] = x_ref[...]

    for load in loads[2:]:
        load.wait()
    rate_ref[...] = -SQUASH_POWER * soft_plus(-rate_ref[...])
    mult_s[...] = jnp.broadcast_to(mult_ref[...].reshape(1, rows), (128, rows)).T[:, 0:1]

    @at_mid
    def _():
        mid_pump(0, 0, PARTS)
        mid_pump(0, 1, 0)
        ag_forward(0)
        ag_finish(0, x_ref)
        normalize(0, 0, nrm)
        lend_rows(0).wait_recv()
        ag_start(layers, agx.at[layers, t], 0)
        mid_pump(0, 2, PARTS)
        for h in range(1, BANDS):
            lend_rows(h).wait_recv()
            ag_start(layers, agx.at[layers, t], h)
        for q in range(PARTS):
            landed(2, mid_block(1), q)
            relay(2, mid_block(1), q, (OUT,))
        own_both(count - 1, OUT)
        ag_forward(layers)
        arrived(0)
        ext[0, 8:] = project(0, nrm).astype(F32)
        send_halo(0)
        for q in range(PARTS):
            landed(1, mid_block(1), q)
            relay(1, mid_block(1), q, mid_ways(1, 1))
            landed(1, mid_block(0), q)
            relay(1, mid_block(0), q, mid_ways(1, 0))
        ag_finish(layers, agx.at[layers, t])
        normalize(layers, 0, nrm_lent)
        lent_out[0] = project(0, nrm_lent)
        lend_back(0).start()
        mid_pump(2, 0, PARTS)
        mid_pump(1, 2, 0)
        for q in range(PARTS):
            relay(2, mid_block(1), q, (ACROSS,))

    @at_end
    def _():
        end_pump(2, 1, 0)
        end_pump(3, 1, 0)
        end_pump(4, 1, 1)
        feed_end(2)
        end_pump(2, 2, 1)
        feed_end(2)
        end_pump(5, 1, 0)
        lend_back(0).wait_recv()
        ext[0, 8:] = lent_in[0].astype(F32)

    take_halo(0)
    gates(0, 0)
    gates(0, 1)
    send_carry(0)

    @at_mid
    def _():
        mid_pump(2, 2, 0, range(PARTS // 2))
        arrived(1)
        lent_out[1] = project(1, nrm_lent)
        lend_back(1).start()
        mid_pump(2, 2, 0, range(PARTS // 2, PARTS))
        gel_s[...] = jax.nn.gelu(project(1, nrm).astype(F32))
        mid_pump(3, 1, 0)
        mid_pump(3, 0, PARTS)

    @at_end
    def _():
        feed_end(4)
        end_pump(2, 3, 0, range(PARTS // 2))
        lend_back(1).wait_recv()
        feed_end(2)
        gel_s[...] = jax.nn.gelu(lent_in[1].astype(F32))

    take_carry(0)
    mix()

    def pieces_of(*runs):
        return [(m, i, q) for m, i, first in runs for q in range(first, PARTS)]

    early = [pieces_of((2, 3, PARTS // 2), (3, 2, 0)) for _ in range(2)]
    final = [pieces_of((4, 3, 0), (5, 2, 0), (5, 3, 0)) for _ in range(2)]

    def end_next(lists, even, odd):
        for parity, steps in ((0, even), (1, odd)):
            now = lists[parity][:steps]
            del lists[parity][:steps]

            @pl.when(is_end & (core == parity))
            def _():
                for m, i, q in now:
                    landed(m, s + inw * i, q)
                    relay(m, s + inw * i, q, (ACROSS,))

    def nothing(_):
        return

    def between(h):
        if h == 0:
            end_do(F(2))
            mid_do(M(3, 2))
        turned = chip == s // (n_tp // chips)
        if h == 0:
            pl.when(is_end & jnp.logical_not(turned))(E(3, 3))
        if h == BANDS - 1:
            pl.when(is_end & turned)(E(3, 3))
            mid_do(M(4, 1), M(4, 0, PARTS))

    def rest_ahead(i, stage):
        even, odd = {
            (1, 0): (0, 1),
            (1, 1): (1, 2),
            (1, 2): (1, 0),
            (2, 0): (0, 1),
            (3, 1): (1, 1),
            (3, 2): (2, 1),
            (3, 3): (1, 0),
        }.get((i, stage), (0, 0))
        end_next(early, even, odd)
        if (i, stage) == (3, 0):
            end_do(F(2))

    project_out(0, rest_ahead)
    close_layer(0, x_ref, between)

    agx[1, t] = xs[1]
    mid_do(M(4, 2), M(5, 0))
    end_do(F(99), E(4, 2))
    end_next(final, 1, 1)
    ag_forward(1)
    end_next(final, 0, 3)
    ag_finish(1, xs.at[1])
    end_next(final, 1, 0)
    normalize(1, 1, nrm)
    end_next(final, 0, 1)
    arrived(3)
    ext[1, 8:] = project(2, nrm).astype(F32)
    send_halo(1)
    mid_do(M(5, 1))
    pl.when(s == 1)(M(5, 2))
    end_next(final, 1, 1)
    take_halo(1)
    end_next(final, 1, 0)
    gates(1, 0)
    end_next(final, 1, 1)
    gates(1, 1)
    send_carry(1)
    pl.when(is_mid & (s > 1))(M(5, 2))
    end_next(final, 1, 1)
    arrived(4)
    end_next(final, 1, 0)
    gel_s[...] = jax.nn.gelu(project(3, nrm).astype(F32))
    end_next(final, 2, 2)
    take_carry(1)
    mix()

    def last_ahead(i, stage):
        even, odd = {(0, 0): (1, 2), (1, 1): (1, 0), (2, 0): (1, 0)}.get((i, stage), (0, 0))
        end_next(final, even, odd)

    project_out(1, last_ahead)
    close_layer(1, xs.at[1], nothing)

    square = jnp.zeros((rows, 1), F32)
    for c in range(2):
        fresh = xs[layers, c].astype(F32)
        square = square + jnp.sum(fresh * fresh, axis=1, keepdims=True)
    sq_out[...] = jnp.broadcast_to(square, (rows, 128)).T[0:8]

    def sq_copy(d):
        return pltpu.make_async_remote_copy(
            src_ref=sq_out,
            dst_ref=sq_in.at[d],
            send_sem=sem_q_send.at[d],
            recv_sem=sem_q_recv.at[d],
            device_id={"tp": lax.rem(t + d, n_tp)},
            device_id_type=MESH,
        )

    for d in range(1, n_tp):
        sq_copy(d).start()
    total = sq_out[0:1]
    for d in range(1, n_tp):
        sq_copy(d).wait_recv()
        total = total + sq_in[d, 0:1]
    inv = lax.rsqrt(total / full + EPSILON)
    inv = jnp.broadcast_to(inv, (128, rows)).T[:, 0:1]
    for c in range(2):
        cols = slice(c * width, (c + 1) * width)
        fresh = xs[layers, c].astype(F32)
        out_ref[:, cols] = (fresh * inv * final_ref[:, cols]).astype(BF16)

    assert not (end_line or mid_in_line or any(early) or any(final))
    close_weights()

    @at_end
    def _():
        for h in range(BANDS):
            lend_rows(h).wait_send()

    @at_mid
    def _():
        ag_close(0)
        ag_close(layers)
        for i in range(len(LENT)):
            lend_back(i).wait_send()

    for layer in range(layers):
        if layer:
            ag_close(layer)

        @pl.when((s >= first_sender(layer)) & (s < n_sp - 1))
        def _():
            halo_copy(layer).wait_send()

        for d in range(1, n_sp):

            @pl.when(s + d < n_sp)
            def _():
                carry_copy(layer, d).wait_send()

        wait_blocks(part.at[layer, pl.ds(0, 2 * chips - 1)], sem_rs_send.at[layer])
    for d in range(1, n_tp):
        sq_copy(d).wait_send()


def in_one_kernel(
    sizes_of,
    starting_stream,
    multiplier_matrix,
    memory_path_matrix,
    filter_coefficients,
    memory_valve_matrix,
    entry_valve_matrix,
    forgetting_parameters,
    timestep_forgetting_multiplier,
    spike_extra,
    exit_projector_matrix,
    prelude_rms_gains,
    finishing_rms_gains,
):
    n_grp, n_sp, n_tp = sizes_of
    rows, feats = starting_stream.shape
    layers, depth, chans = memory_path_matrix.shape
    pieces = rows // 128 if rows % 128 == 0 else 1
    sizes = (layers, n_sp, n_tp, n_grp, rows, chans, feats, depth, pieces)
    chips = n_tp // 2
    half_in = (layers, 2, depth // 2, chans)
    vmem = pl.BlockSpec(memory_space=pltpu.VMEM)
    hbm = pl.BlockSpec(memory_space=pl.ANY)
    count = 3 * layers
    dma = pltpu.SemaphoreType.DMA
    return pl.pallas_call(
        functools.partial(fused, sizes),
        out_shape=jax.ShapeDtypeStruct((rows, feats), BF16),
        in_specs=[hbm] * 12,
        out_specs=vmem,
        scratch_shapes=[
            pltpu.VMEM((2, rows, feats // 2), BF16),
            pltpu.VMEM(filter_coefficients.shape, BF16),
            pltpu.VMEM(memory_valve_matrix.shape, BF16),
            pltpu.VMEM(entry_valve_matrix.shape, BF16),
            pltpu.VMEM((layers, chans), F32),
            pltpu.VMEM((rows,), F32),
            pltpu.VMEM((rows, chans), F32),
            pltpu.VMEM((layers, n_tp * feats), F32),
            pltpu.VMEM((1, feats), F32),
            pltpu.VMEM((2 * layers * n_sp * 2, depth // 2, chans), BF16),
            pltpu.VMEM((layers * n_sp * 2, chans, depth // 2), BF16),
            pltpu.VMEM((layers + 1, n_tp, 2, rows, feats // 2), BF16),
            pltpu.VMEM((layers + 1, 2, rows, feats // 2), BF16),
            pltpu.VMEM((rows, n_tp * feats), BF16),
            pltpu.VMEM((rows, n_tp * feats), BF16),
            pltpu.VMEM((layers, 8 + rows, chans), F32),
            pltpu.VMEM((layers, 8, chans), F32),
            pltpu.VMEM((rows, chans), F32),
            pltpu.VMEM((rows, chans), F32),
            pltpu.VMEM((rows, chans), F32),
            pltpu.VMEM((rows, chans), BF16),
            pltpu.VMEM((len(LENT), rows, chans), BF16),
            pltpu.VMEM((len(LENT), rows, chans), BF16),
            pltpu.VMEM((layers, n_tp, 2, rows, feats // 2), BF16),
            pltpu.VMEM((layers, chips, 2, rows, feats // 2), BF16),
            pltpu.VMEM((layers, chips, 2, rows, feats // 2), BF16),
            pltpu.VMEM((layers, chips, 2, rows, feats // 2), BF16),
            pltpu.VMEM((layers, 2, chans), F32),
            pltpu.VMEM((layers, n_sp, 2, chans), F32),
            pltpu.VMEM((1, chans), F32),
            pltpu.VMEM((rows, 1), F32),
            pltpu.VMEM((8, rows), F32),
            pltpu.VMEM((n_tp, 8, rows), F32),
            dma((10,)),
            dma((count, 2)),
            dma((count, n_sp - 1, PARTS)),
            dma((count, n_sp - 1)),
            dma((3,)),
            dma((BANDS + 2 * len(LENT),)),
            dma((layers + 1,)),
            dma((layers + 1, n_tp, BANDS)),
            dma((layers,)),
            dma((layers, 2 * chips - 1, BANDS)),
            dma((layers, 2)),
            dma((layers, n_sp)),
            dma((layers, n_sp)),
            dma((n_tp,)),
            dma((n_tp,)),
        ],
        compiler_params=pltpu.CompilerParams(
            collective_id=0, has_side_effects=True, vmem_limit_bytes=60 * 2**20
        ),
    )(
        starting_stream,
        multiplier_matrix.reshape(half_in),
        memory_path_matrix.reshape(half_in),
        exit_projector_matrix,
        filter_coefficients,
        memory_valve_matrix,
        entry_valve_matrix,
        forgetting_parameters,
        timestep_forgetting_multiplier,
        spike_extra,
        prelude_rms_gains,
        finishing_rms_gains.reshape(1, feats),
    )


def on_each(sizes_of, *arrays):
    stream, memory = arrays[0], arrays[2]
    n_grp, n_sp, n_tp = sizes_of
    rows, feats = stream.shape
    depth, chans = memory.shape[1:]
    fits = (
        n_grp == 2
        and n_sp == 4
        and memory.shape[0] == 2
        and n_tp % 2 == 0
        and rows % 128 == 0
        and depth % 128 == 0
        and feats % 256 == 0
        and chans % BLOCK_W == 0
        and depth == feats
        and n_sp == n_tp
    )
    if fits:
        return in_one_kernel(sizes_of, *arrays)
    return on_device(*arrays)


def solution(mesh):
    sizes_of = tuple(mesh.shape[axis] for axis in ("grp", "sp", "tp"))
    body = functools.partial(on_each, sizes_of)
    return jax.shard_map(
        body,
        mesh=mesh,
        in_specs=(
            P(("grp", "sp"), "tp"),
            P(None, "sp", "tp"),
            P(None, "sp", "tp"),
            P(None, None, "tp"),
            P(None, "tp", None, None),
            P(None, "tp", None, None),
            P(None, "tp"),
            P(("grp", "sp")),
            P(("grp", "sp"), "tp"),
            P(None, "tp", "sp"),
            P(),
            P("tp"),
        ),
        out_specs=P(("grp", "sp"), "tp"),
        check_vma=False,
    )
```
